256 devices in a mesh: ep: 64 (over z, y, core), tp: 4 (over x).
Axes of the slice: x: 4, y: 4, z: 8, core: 2. Of those that a mesh axis runs over, the one named last changes fastest.
Arguments:
- tokens: bfloat16 [2048, 2048], P('ep', 'tp'), may hold values from -33 to 33
- previous: bfloat16 [2048, 2048], P('ep', 'tp'), may hold values from -6 to 6
- first_norm_gain: float32 [2048], replicated, may hold values from 0.1 to 1.9
- token_shift_share: float32 [5, 2048], replicated, may hold values from 0 to 1
- receptance_weight: bfloat16 [2048, 1024], P(None, 'tp'), may hold values from -0.125 to 0.125
- key_weight: bfloat16 [2048, 1024], P(None, 'tp'), may hold values from -0.125 to 0.125
- value_weight: bfloat16 [2048, 1024], P(None, 'tp'), may hold values from -0.125 to 0.125
- decay_down_map: bfloat16 [2048, 128], replicated, may hold values from -0.125 to 0.125
- decay_up_map: bfloat16 [128, 1024], replicated, may hold values from -0.5 to 0.5
- decay_offset: float32 [1024], P('tp'), may hold values from -4 to 1
- strength_down_map: bfloat16 [2048, 128], replicated, may hold values from -0.125 to 0.125
- strength_up_map: bfloat16 [128, 1024], replicated, may hold values from -0.5 to 0.5
- removal_key_scale: float32 [1024], P('tp'), may hold values from 0.3 to 3
- key_damping: float32 [1024], P('tp'), may hold values from 0.1 to 1.9
- self_term_weight: float32 [16, 64], P('tp'), may hold values from -0.6 to 0.6
- head_norm_gain: float32 [1024], P('tp'), may hold values from 0.1 to 1.9
- output_weight: bfloat16 [1024, 2048], P('tp'), may hold values from -0.1875 to 0.1875
- state: float32 [2048, 16, 64, 64], P('ep', 'tp'), may hold values from -6 to 6
- second_norm_gain: float32 [2048], replicated, may hold values from 0.1 to 1.9
- routes: int32 [2048, 4], P('ep'), may hold values from 0 to 63, all different within a row; in each aligned block of 32 rows (0 to 31, 32 to 63, ...) at most 3 rows name the same one
- chosen_expert_weight: float32 [2048, 4], P('ep'), may hold values from 0.1 to 1
- expert_gate_weight: bfloat16 [64, 2048, 1024], P('ep', None, 'tp'), may hold values from -0.5 to 0.5
- expert_up_weight: bfloat16 [64, 2048, 1024], P('ep', None, 'tp'), may hold values from -0.5 to 0.5
- expert_down_weight: bfloat16 [64, 1024, 2048], P('ep', 'tp'), may hold values from -0.046875 to 0.046875
Outputs:
- layer_out: bfloat16 [2048, 2048], P('ep', 'tp')
- new_state: float32 [2048, 16, 64, 64], P('ep', 'tp')
The draws below stay inside these ranges and needn't reach their ends.
Inputs may be any that keep to these rules, and one draw needn't show every extreme that they name: `routes`: each row names 4 different experts. Among the rows of one index of ep no expert is named by more than 3 rows, and in every draw some expert is named by exactly 3 rows of some index of ep.
All inputs are finite; a program needn't handle non-finite values.
Results may differ from the reference program's by a relative error of at most 0.015.
Values may be sent and summed in bfloat16 or wider, within the bound.
A program may use at most 64 MiB of HBM per device.

```python
import math
import jax
import jax.numpy as jnp
import numpy as np
from jax import lax

D = 2048
HEAD_TOTAL = 16
HEAD_WIDTH = 64
DECAY_RANK = 128
ALPHA_RANK = 128
FF = 1024
TOP_K = 4
SEQ_DEV = 32
SEQS = 2048
EXPERTS = 64
CAP = 3
N_EP = 64
N_TP = 4


def draw_tokens(key, part):
    row_key = jax.random.fold_in(key, 11)
    col_key = jax.random.fold_in(key, 12)
    base_key = jax.random.fold_in(key, 13)
    row_scales = jnp.exp(jax.random.uniform(row_key, (SEQS, 1), jnp.float32, -0.69, 0.69))
    ramp = jnp.exp((jnp.arange(D, dtype=jnp.float32) / D - 0.5) * 1.0986)
    col_scales = jnp.exp(jax.random.uniform(col_key, (1, D), jnp.float32, -1.15, 1.15)) * ramp[None, :]
    base = jnp.clip(jax.random.normal(base_key, (SEQS, D), jnp.float32), -3.0, 3.0)
    return (base * row_scales * col_scales).astype(jnp.bfloat16)


def block_levels(stream_key, extent, pieces, low, top_value):
    loudness, own = 1.0, jax.random.fold_in(stream_key, 6)
    for axis_at, shards_of in pieces:
        steps = jnp.exp(jax.random.uniform(jax.random.fold_in(own, axis_at), (shards_of,), jnp.float32, low / len(pieces), top_value / len(pieces)))
        loudness = loudness * jnp.repeat(steps, extent[axis_at] // shards_of).reshape([-1 if axis == axis_at else 1 for axis in range(len(extent))])
    return loudness


def assign_block(key, own, number, rows, count, top, reach, skew):
    order = jax.random.permutation(key, count)
    crowded, usual = portions_of(count, rows * top, reach, skew, True), portions_of(count, rows * top, reach, skew, False)
    places = jnp.arange(count)

    def named(tallies, turn):
        used = int((tallies > 0).sum())
        fixed = max(1, used // 4)
        passed = fixed + (places - fixed + turn * (used - fixed)) % max(1, count - fixed)
        return jnp.zeros((count,), jnp.int32).at[order[jnp.where(places < fixed, places, passed)]].set(jnp.asarray(tallies, jnp.int32))

    tallies = jnp.where(number % 4 == 0, named(crowded, number // 4), named(usual, number - number // 4 - 1))
    mixed = jax.random.permutation(jax.random.fold_in(own, 3), count)
    giver, sink = mixed[0:count // 2 * 2:2], mixed[1:count // 2 * 2:2]
    room = jnp.minimum(tallies[giver] - 1, reach - tallies[sink]) // 2
    room = jnp.where((giver == order[0]) | (sink == order[0]) | (tallies[sink] == 0), 0, jnp.maximum(room, 0))
    passed = jax.random.randint(jax.random.fold_in(own, 4), (count // 2,), 0, 1 << 20) % (room + 1)
    tallies = tallies.at[giver].add(-passed).at[sink].add(passed)
    labels = jnp.searchsorted(jnp.cumsum(tallies), jnp.arange(rows * top), side="right").astype(jnp.int32)
    table = labels.reshape(top, rows).T
    table = table[jax.random.permutation(jax.random.fold_in(own, 1), rows)]
    turn = jax.random.randint(jax.random.fold_in(own, 2), (rows, 1), 0, top)
    return jnp.take_along_axis(table, (jnp.arange(top)[None, :] + turn) % top, axis=1)


def portions_of(number_of, total, reach, slope, full):
    weights = [(1 << 20) // math.isqrt(grade ** slope) + 1 for grade in range(1, number_of + 1)]
    largest = reach if full else min(reach, max(-(-total // number_of), total * weights[0] // sum(weights)))
    least = 1 if total - largest >= number_of - 1 else 0
    holding, rest = [largest] + [least] * (number_of - 1), total - largest - least * (number_of - 1)
    while rest > 0:
        free = [i for i in range(1, number_of) if holding[i] < largest] or [i for i in range(1, number_of) if holding[i] < reach]
        mass, left = sum([weights[i] for i in free]), rest
        for i in free:
            extra = min(reach - holding[i], max(1, left * weights[i] // mass), rest)
            holding[i] = holding[i] + extra
            rest = rest - extra
    return np.array(holding)


def centred(key, shape, deviation, most, cuts=(), kind=jnp.bfloat16):
    result = jax.random.normal(key, shape, jnp.float32) * deviation
    if len(cuts) > 0:
        result = block_levels(key, shape, cuts, -0.22, 0.18) * result
    return jnp.clip(result, min=-most, max=most).astype(kind)


def setup_inputs(seed: int = 0) -> dict:
    key_list = jax.random.split(jax.random.key(seed), 25)
    tokens = draw_tokens(jax.random.fold_in(key_list[24], 71), 0)
    previous = centred(key_list[1], (SEQS, D), 1.0, 6.0, ((0, 64), (1, 4)))
    first_norm_gain = jnp.clip(1.0 + 0.18 * jax.random.normal(key_list[2], (D,), jnp.float32), 0.1, 1.9)
    token_shift_share = jnp.clip(jax.random.uniform(key_list[3], (5, D), jnp.float32, 0.0, 1.0), 0.0, 1.0)
    receptance_weight = centred(key_list[4], (D, HEAD_TOTAL * HEAD_WIDTH), D ** -0.5, 0.125, ((1, 4),))
    key_weight = centred(key_list[5], (D, HEAD_TOTAL * HEAD_WIDTH), D ** -0.5, 0.125, ((1, 4),))
    value_weight = centred(key_list[6], (D, HEAD_TOTAL * HEAD_WIDTH), D ** -0.5, 0.125, ((1, 4),))
    decay_down_map = centred(key_list[7], (D, DECAY_RANK), D ** -0.5, 0.125)
    decay_up_map = centred(key_list[8], (DECAY_RANK, HEAD_TOTAL * HEAD_WIDTH), DECAY_RANK ** -0.5, 0.5)
    decay_offset = jnp.clip(-4.0 + 5.0 * jax.random.uniform(key_list[9], (HEAD_TOTAL * HEAD_WIDTH,), jnp.float32) ** block_levels(key_list[9], (HEAD_TOTAL * HEAD_WIDTH,), ((0, 4),), -0.2, 0.2), -4.0, 1.0)
    strength_down_map = centred(key_list[10], (D, ALPHA_RANK), D ** -0.5, 0.125)
    strength_up_map = centred(key_list[11], (ALPHA_RANK, HEAD_TOTAL * HEAD_WIDTH), ALPHA_RANK ** -0.5, 0.5)
    removal_key_scale = jnp.clip(jnp.exp(math.log(3.0) - 2.3025851 * jax.random.uniform(key_list[12], (HEAD_TOTAL * HEAD_WIDTH,), jnp.float32) ** block_levels(key_list[12], (HEAD_TOTAL * HEAD_WIDTH,), ((0, 4),), -0.2, 0.2)), 0.3, 3.0)
    key_damping = jnp.clip(1.0 + 0.18 * jax.random.normal(key_list[13], (HEAD_TOTAL * HEAD_WIDTH,), jnp.float32), 0.1, 1.9)
    self_term_weight = centred(key_list[14], (HEAD_TOTAL, HEAD_WIDTH), 0.1, 0.6, ((0, 4),), jnp.float32)
    head_norm_gain = jnp.clip(1.0 + 0.18 * jax.random.normal(key_list[15], (HEAD_TOTAL * HEAD_WIDTH,), jnp.float32), 0.1, 1.9)
    output_weight = centred(key_list[16], (HEAD_TOTAL * HEAD_WIDTH, D), (HEAD_TOTAL * HEAD_WIDTH) ** -0.5, 0.1875, ((0, 4),))
    state = centred(key_list[17], (SEQS, HEAD_TOTAL, HEAD_WIDTH, HEAD_WIDTH), 1.0, 6.0, ((0, 64), (1, 4)), jnp.float32)
    second_norm_gain = jnp.clip(1.0 + 0.18 * jax.random.normal(key_list[18], (D,), jnp.float32), 0.1, 1.9)
    routes_keys = jax.random.split(jax.random.fold_in(key_list[19], 1), SEQS // SEQ_DEV)
    routes_turns = jax.random.permutation(jax.random.fold_in(key_list[19], 3), SEQS // SEQ_DEV)
    routes = jax.vmap(lambda own, number: assign_block(jax.random.fold_in(key_list[19], 2), own, number, SEQ_DEV, EXPERTS, TOP_K, CAP, 2))(routes_keys, routes_turns).reshape((SEQS, TOP_K))
    chosen_expert_weight = jnp.clip(jnp.exp(math.log(1.0) - 2.3025851 * jax.random.uniform(key_list[20], (SEQS, TOP_K), jnp.float32) ** block_levels(key_list[20], (SEQS, TOP_K), ((0, 64),), -0.2, 0.2)), 0.1, 1.0)
    expert_gate_weight = centred(key_list[21], (EXPERTS, D, FF), (D // 16) ** -0.5, 0.5, ((0, 64), (2, 4)))
    expert_up_weight = centred(key_list[22], (EXPERTS, D, FF), (D // 16) ** -0.5, 0.5, ((0, 64), (2, 4)))
    expert_down_weight = centred(key_list[23], (EXPERTS, FF, D), (16 * FF) ** -0.5, 0.046875, ((0, 64), (1, 4)))
    return {"tokens": tokens, "previous": previous, "first_norm_gain": first_norm_gain, "token_shift_share": token_shift_share, "receptance_weight": receptance_weight, "key_weight": key_weight, "value_weight": value_weight, "decay_down_map": decay_down_map, "decay_up_map": decay_up_map, "decay_offset": decay_offset, "strength_down_map": strength_down_map, "strength_up_map": strength_up_map, "removal_key_scale": removal_key_scale, "key_damping": key_damping, "self_term_weight": self_term_weight, "head_norm_gain": head_norm_gain, "output_weight": output_weight, "state": state, "second_norm_gain": second_norm_gain, "routes": routes, "chosen_expert_weight": chosen_expert_weight, "expert_gate_weight": expert_gate_weight, "expert_up_weight": expert_up_weight, "expert_down_weight": expert_down_weight}


NORM_EPS = 1e-06
GROUP_EPS = 0.00064
KEY_EPS = 1e-06
GATE_LIMIT = 7.0
GATE_SLOPE = 1.702

def row_rescale(values, gain):
    return values * lax.rsqrt(lax.optimization_barrier(jnp.mean(values * values, axis=-1, keepdims=True)) + NORM_EPS) * gain

def head_combiner(present_rows, prior_rows, first_norm_gain, token_shift_share, receptance_weight, key_weight, value_weight, decay_down_map, decay_up_map, decay_offset, strength_down_map, strength_up_map, removal_key_scale, key_damping, self_term_weight, head_norm_gain, state):
    sequence_count = present_rows.shape[0]
    head_number = state.shape[1]
    head_extent = state.shape[2]
    normed = row_rescale(present_rows.astype(jnp.float32), first_norm_gain)
    before = prior_rows.astype(jnp.float32)

    def shifted(role):
        return (normed + (before - normed) * token_shift_share[role]).astype(jnp.bfloat16)

    def project(inputs, weight):
        return jnp.dot(inputs, weight, preferred_element_type=jnp.float32)

    def by_heads(values):
        return values.reshape(sequence_count, head_number, head_extent)
    receptance_rows = by_heads(project(shifted(0), receptance_weight))
    key_rows = by_heads(project(shifted(1), key_weight))
    value_matrix = by_heads(project(shifted(2), value_weight))
    decay_low = jnp.tanh(project(shifted(3), decay_down_map)).astype(jnp.bfloat16)
    decay_pre = decay_offset + project(decay_low, decay_up_map)
    decay = by_heads(jnp.exp(-jnp.exp(-jax.nn.softplus(-decay_pre) - 0.5)))
    alpha_low = project(shifted(4), strength_down_map).astype(jnp.bfloat16)
    alpha = by_heads(jax.nn.sigmoid(project(alpha_low, strength_up_map)))
    removal = key_rows * removal_key_scale.reshape(head_number, head_extent)
    removal = removal * lax.rsqrt(lax.optimization_barrier(jnp.sum(removal * removal, axis=-1, keepdims=True)) + KEY_EPS)
    blended_rows = key_rows * (1.0 + (alpha - 1.0) * key_damping.reshape(head_number, head_extent))
    highest = lax.Precision.HIGHEST
    along = jnp.einsum('shij,shj->shi', state, removal, precision=highest)
    new_state = state * decay[:, :, None, :] - along[..., None] * (removal * alpha)[:, :, None, :] + value_matrix[..., None] * blended_rows[:, :, None, :]
    readout = jnp.einsum('shij,shj->shi', new_state, receptance_rows, precision=highest)
    centered = readout - lax.optimization_barrier(jnp.mean(readout, axis=-1, keepdims=True))
    variance = lax.optimization_barrier(jnp.mean(centered * centered, axis=-1, keepdims=True))
    heads_normalised = centered * lax.rsqrt(variance + GROUP_EPS) * head_norm_gain.reshape(head_number, head_extent)
    self_term = lax.optimization_barrier(jnp.sum(receptance_rows * blended_rows * self_term_weight, axis=-1, keepdims=True)) * value_matrix
    mixed_inputs = (heads_normalised + self_term).reshape(sequence_count, head_number * head_extent).astype(jnp.bfloat16)
    return (mixed_inputs, new_state)

def split_sum(left, right):
    block_rows = left.shape[1] // N_TP
    total = jnp.zeros((left.shape[0], right.shape[1]), jnp.float32)
    for block_index in range(N_TP):
        lower = block_index * block_rows
        product = jnp.dot(left[:, lower:lower + block_rows], right[lower:lower + block_rows], preferred_element_type=jnp.float32).astype(jnp.bfloat16)
        total = total + lax.optimization_barrier(product).astype(jnp.float32)
    return total

def reference(tokens, previous, first_norm_gain, token_shift_share, receptance_weight, key_weight, value_weight, decay_down_map, decay_up_map, decay_offset, strength_down_map, strength_up_map, removal_key_scale, key_damping, self_term_weight, head_norm_gain, output_weight, state, second_norm_gain, routes, chosen_expert_weight, expert_gate_weight, expert_up_weight, expert_down_weight):
    model_width = tokens.shape[1]

    def one_group(blocks):
        present_rows, prior_rows, state_tile = blocks
        return head_combiner(present_rows, prior_rows, first_norm_gain, token_shift_share, receptance_weight, key_weight, value_weight, decay_down_map, decay_up_map, decay_offset, strength_down_map, strength_up_map, removal_key_scale, key_damping, self_term_weight, head_norm_gain, state_tile)
    mixed_inputs, new_state = lax.map(one_group, (tokens.reshape(N_EP, SEQ_DEV, model_width), previous.reshape(N_EP, SEQ_DEV, model_width), state.reshape(N_EP, SEQ_DEV, HEAD_TOTAL, HEAD_WIDTH, HEAD_WIDTH)))
    mixed_inputs = mixed_inputs.reshape(SEQS, HEAD_TOTAL * HEAD_WIDTH)
    new_state = new_state.reshape(SEQS, HEAD_TOTAL, HEAD_WIDTH, HEAD_WIDTH)
    residual = tokens.astype(jnp.float32) + split_sum(mixed_inputs, output_weight)
    expert_in = row_rescale(residual, second_norm_gain).astype(jnp.bfloat16)
    grouped = routes.reshape(N_EP, SEQ_DEV * TOP_K)
    expert_ids = jnp.arange(EXPERTS, dtype=jnp.int32)
    onehot = (grouped[:, :, None] == expert_ids[None, None, :]).astype(jnp.int32)
    ranking = lax.optimization_barrier(jnp.sum((jnp.cumsum(onehot, axis=1) - onehot) * onehot, axis=2))
    source = jnp.arange(N_EP, dtype=jnp.int32)[:, None]
    slot_index = (grouped * (N_EP * CAP) + source * CAP + ranking).reshape(-1).astype(jnp.int32)
    owner = (jnp.arange(SEQS * TOP_K, dtype=jnp.int32) // TOP_K).astype(jnp.int32)
    buffer = jnp.zeros((EXPERTS * N_EP * CAP, model_width), jnp.bfloat16).at[slot_index].set(expert_in[owner])

    def one_expert(blocks):
        rows_in, gate_weight, up_weight, down_weight = blocks
        gate_pre = jnp.minimum(jnp.dot(rows_in, gate_weight, preferred_element_type=jnp.float32), GATE_LIMIT)
        up_pre = jnp.clip(jnp.dot(rows_in, up_weight, preferred_element_type=jnp.float32), -GATE_LIMIT, GATE_LIMIT)
        activation = ((up_pre + 1.0) * gate_pre * jax.nn.sigmoid(GATE_SLOPE * gate_pre)).astype(jnp.bfloat16)
        return split_sum(activation, down_weight).astype(jnp.bfloat16)
    expert_out = lax.map(one_expert, (buffer.reshape(EXPERTS, N_EP * CAP, model_width), expert_gate_weight, expert_up_weight, expert_down_weight))
    picked = expert_out.reshape(EXPERTS * N_EP * CAP, model_width)[slot_index].astype(jnp.float32)
    picked = picked.reshape(SEQS, TOP_K, model_width)
    layer_out = (residual + lax.optimization_barrier(jnp.sum(picked * chosen_expert_weight[:, :, None], axis=1))).astype(jnp.bfloat16)
    return (layer_out, new_state)
```

```python
import jax
import jax.numpy as jnp
from jax import lax
from jax.experimental import pallas as pl
from jax.experimental.pallas import tpu as pltpu
from jax.sharding import PartitionSpec as P

NORM_EPS = 1e-06
GROUP_EPS = 0.00064
KEY_EPS = 1e-06
GATE_LIMIT = 7.0
GATE_SLOPE = 1.702


def in_one_piece(arrays, axis, dim, along):
    widths = [a.shape[along] for a in arrays]
    both = jnp.concatenate(arrays, axis=along)
    result = lax.all_gather(both, axis, axis=dim, tiled=True)
    return tuple(jnp.split(result, [sum(widths[:k]) for k in range(1, len(widths))], axis=along))


def row_rescale(values, gain):
    return values * lax.rsqrt(jnp.mean(values * values, axis=-1, keepdims=True) + NORM_EPS) * gain


def head_combiner(
    present_rows,
    prior_rows,
    first_norm_gain,
    token_shift_share,
    receptance_weight,
    key_weight,
    value_weight,
    decay_down_map,
    decay_up_map,
    decay_offset,
    strength_down_map,
    strength_up_map,
    removal_key_scale,
    key_damping,
    self_term_weight,
    head_norm_gain,
    state,
):
    sequence_count = present_rows.shape[0]
    head_number = state.shape[1]
    head_extent = state.shape[2]
    normed = row_rescale(present_rows.astype(jnp.float32), first_norm_gain)
    before = prior_rows.astype(jnp.float32)

    def shifted(role):
        return (normed + (before - normed) * token_shift_share[role]).astype(jnp.bfloat16)

    def project(inputs, weight):
        return jnp.dot(inputs, weight, preferred_element_type=jnp.float32)

    def by_heads(values):
        return values.reshape(sequence_count, head_number, head_extent)

    receptance_rows = by_heads(project(shifted(0), receptance_weight))
    key_rows = by_heads(project(shifted(1), key_weight))
    value_matrix = by_heads(project(shifted(2), value_weight))
    decay_low = jnp.tanh(project(shifted(3), decay_down_map)).astype(jnp.bfloat16)
    decay_pre = decay_offset + project(decay_low, decay_up_map)
    decay = by_heads(jnp.exp(-jnp.exp(-jax.nn.softplus(-decay_pre) - 0.5)))
    alpha_low = project(shifted(4), strength_down_map).astype(jnp.bfloat16)
    alpha = by_heads(jax.nn.sigmoid(project(alpha_low, strength_up_map)))
    removal = key_rows * removal_key_scale.reshape(head_number, head_extent)
    removal = removal * lax.rsqrt(jnp.sum(removal * removal, axis=-1, keepdims=True) + KEY_EPS)
    blended_rows = key_rows * (1.0 + (alpha - 1.0) * key_damping.reshape(head_number, head_extent))
    along = jnp.einsum("shij,shj->shi", state, removal)
    new_state = (
        state * decay[:, :, None, :]
        - along[..., None] * (removal * alpha)[:, :, None, :]
        + value_matrix[..., None] * blended_rows[:, :, None, :]
    )
    readout = jnp.einsum("shij,shj->shi", new_state, receptance_rows)
    centered = readout - jnp.mean(readout, axis=-1, keepdims=True)
    variance = jnp.mean(centered * centered, axis=-1, keepdims=True)
    heads_normalised = (
        centered
        * lax.rsqrt(variance + GROUP_EPS)
        * head_norm_gain.reshape(head_number, head_extent)
    )
    self_term = (
        jnp.sum(receptance_rows * blended_rows * self_term_weight, axis=-1, keepdims=True)
        * value_matrix
    )
    mixed_inputs = (
        (heads_normalised + self_term)
        .reshape(sequence_count, head_number * head_extent)
        .astype(jnp.bfloat16)
    )
    return (mixed_inputs, new_state)


MESH = pl.DeviceIdType.MESH
N_EP = 64
N_TP = 4
GROUPS = 4
NS = N_EP // GROUPS
ORDER = (0, 3, 1, 2)
SLOTS = 3
KEPT = 4 * SLOTS * NS
PACKED = KEPT + NS
F32 = jnp.float32
BF16 = jnp.bfloat16


def dot(a, b):
    return jnp.dot(a, b, preferred_element_type=F32)


def iota(shape, dim):
    return lax.broadcasted_iota(jnp.int32, shape, dim)


def third(m):
    return (m * 11) >> 5


def kept_row(m):
    return jnp.where(m == 12, 3, m + third(m))


def tail_kernel(
    mixed_ref, tokens_ref, gain_ref, routes_ref, routes_row_ref, routes_tiled_ref, weight_ref,
    wout_hbm, wg_hbm, wu_hbm, wd_hbm,
    out_ref,
    wout, wg, wu, wd, place, take, pick, unpick,
    rs_send, rs_recv, residual, send_a, recv_a, gathered, down_send, down_recv, send_b, recv_b,
    w_sem, rs_ssem, rs_rsem, a_ssem, a_rsem, g_ssem, g_rsem, d_ssem, d_rsem, b_ssem, b_rsem,
):
    me = lax.axis_index("ep")
    tp = lax.axis_index("tp")
    loads = [
        pltpu.make_async_copy(wout_hbm, wout, w_sem.at[0]),
        pltpu.make_async_copy(wg_hbm.at[0], wg, w_sem.at[1]),
        pltpu.make_async_copy(wu_hbm.at[0], wu, w_sem.at[2]),
        pltpu.make_async_copy(wd_hbm.at[0], wd, w_sem.at[3]),
    ]
    for load in loads:
        load.start()
    barrier = pltpu.get_barrier_semaphore()
    for d in range(1, N_TP):
        pl.semaphore_signal(
            barrier, inc=1, device_id={"tp": lax.rem(tp + d, N_TP)}, device_id_type=MESH
        )

    def greet(d, carry):
        pl.semaphore_signal(
            barrier, inc=1, device_id={"ep": lax.rem(me + d, N_EP)}, device_id_type=MESH
        )
        return carry

    lax.fori_loop(1, N_EP, greet, 0)

    loads[0].wait()
    for j in range(N_TP):
        rs_send[j] = dot(mixed_ref[...], wout[:, j * 512 : (j + 1) * 512]).astype(BF16)
    pl.semaphore_wait(barrier, N_EP - 1 + N_TP - 1)
    rs_copies = []
    for d in (2, 1, 3):
        peer = lax.rem(tp + d, N_TP)
        copy = pltpu.make_async_remote_copy(
            src_ref=rs_send.at[peer], dst_ref=rs_recv.at[d - 1],
            send_sem=rs_ssem.at[d - 1], recv_sem=rs_rsem.at[d - 1],
            device_id={"tp": peer}, device_id_type=MESH,
        )
        copy.start()
        rs_copies.append(copy)

    lane = iota((1, 256), 1)
    block, seq = lane // 32, lane % 32
    source = iota((32, 256), 0)
    targets = []
    for c in range(4):
        mine = routes_tiled_ref[c : c + 1, :]
        rank = jnp.zeros((1, 256), jnp.int32)
        for other in range(c + 1):
            same = routes_ref[:, other : other + 1] == mine
            if other == c:
                same = same & (source < seq)
            rank = rank + jnp.sum(same.astype(jnp.int32), axis=0, keepdims=True)
        row = jnp.where(block < 4, block * 4 + rank, jnp.where(rank == block - 4, 3, -4096))
        targets.append(mine * 16 + row)

    def fill_place(i, carry):
        at = pl.multiple_of(i * 128, 128)
        row = iota((128, 256), 0) + at
        hit = row == targets[0]
        for c in range(1, 4):
            hit = hit | (row == targets[c])
        place[pl.ds(at, 128), :] = hit.astype(F32).astype(BF16)
        return carry

    lax.fori_loop(0, 8, fill_place, 0)

    piece, tile_row = iota((PACKED, 16 * NS), 0), iota((PACKED, 16 * NS), 1)
    pick[...] = (tile_row == (piece % NS) * 16 + kept_row(piece // NS)).astype(F32).astype(BF16)
    tile_row, piece = iota((16 * NS, KEPT), 0), iota((16 * NS, KEPT), 1)
    unpick[...] = (tile_row == (piece % NS) * 16 + kept_row(piece // NS)).astype(F32).astype(BF16)

    for copy in rs_copies:
        copy.wait()
    total = tokens_ref[...].astype(F32) + rs_send[tp].astype(F32)
    for d in range(N_TP - 1):
        total = total + rs_recv[d].astype(F32)
    residual[...] = total
    square = jnp.sum(total * total, axis=1, keepdims=True)
    high = square.astype(BF16).astype(F32)
    low = square - high
    scaled = total * gain_ref[pl.ds(tp, 1), :]
    stack = [scaled[:, k * 128 : (k + 1) * 128] for k in range(4)]
    sum_lane = iota((32, 128), 1)
    for j in range(SLOTS):
        stack.append(jnp.where(sum_lane == j, high, jnp.where(sum_lane == 3 + j, low, 0.0)))
    stack.append(jnp.zeros((32, 128), F32))
    stack = jnp.concatenate(stack, axis=0).astype(BF16)
    send_a[...] = dot(place[...], stack).astype(BF16).reshape(N_EP, 16, 128)

    def out_copy(r, group):
        peer = lax.rem(me + N_EP - r, N_EP)
        return pltpu.make_async_remote_copy(
            src_ref=send_a.at[peer], dst_ref=recv_a.at[r],
            send_sem=a_ssem, recv_sem=a_rsem.at[group],
            device_id={"ep": peer}, device_id_type=MESH,
        )

    for group in ORDER:

        def send_out(r, carry, group=group):
            out_copy(r, group).start()
            return carry

        lax.fori_loop(max(1, group * NS), (group + 1) * NS, send_out, 0)
    recv_a[0] = send_a[me]

    seq_col = iota((32, 128), 0)
    earlier = iota((32, 128), 1)
    columns = []
    for c in range(4):
        mine = routes_ref[:, c : c + 1]
        same = (routes_row_ref[...] == mine) & (earlier < c * 32 + seq_col)
        columns.append(mine * 16 + jnp.sum(same.astype(jnp.int32), axis=1, keepdims=True))
    for k in range(4):
        for j in range(8):
            at = iota((32, 128), 1) + (j * 128 - k * 4)
            share = jnp.zeros((32, 128), F32)
            for c in range(4):
                share = jnp.where(at == columns[c], weight_ref[:, c : c + 1], share)
            upper = share.astype(BF16)
            take[k * 32 : (k + 1) * 32, j * 128 : (j + 1) * 128] = upper
            take[128 + k * 32 : 160 + k * 32, j * 128 : (j + 1) * 128] = (
                share - upper.astype(F32)
            ).astype(BF16)

    def wait_bytes(ref, sem):
        pltpu.make_async_copy(ref, ref, sem).wait()

    g_copies = []
    for n, group in enumerate(ORDER):
        first = group * NS
        count = NS - 1 if group == 0 else NS
        wait_bytes(recv_a.at[pl.ds(first, count)], a_rsem.at[group])
        tiles = recv_a[first : first + NS].reshape(NS * 16, 128)
        gathered[n, tp] = dot(pick[...], tiles).astype(BF16)
        for d in (2, 1, 3):
            copy = pltpu.make_async_remote_copy(
                src_ref=gathered.at[n, tp], dst_ref=gathered.at[n, tp],
                send_sem=g_ssem.at[n, d - 1], recv_sem=g_rsem.at[n, d - 1],
                device_id={"tp": lax.rem(tp + d, N_TP)}, device_id_type=MESH,
            )
            copy.start()
            g_copies.append(copy)
    for load in loads[1:]:
        load.wait()
    d_copies = []
    for n, group in enumerate(ORDER):
        for copy in g_copies[3 * n : 3 * n + 3]:
            copy.wait_recv()
        rows, sums = [], None
        for t in range(N_TP):
            for k in range(4):
                rows.append(gathered[n, t, k * 3 * NS : (k + 1) * 3 * NS, :])
            part = gathered[n, t, KEPT:PACKED, :].astype(F32)
            sums = part if sums is None else sums + part
        rows = jnp.concatenate(rows, axis=1)
        square = jnp.concatenate(
            [sums[:, j : j + 1] + sums[:, 3 + j : 4 + j] for j in range(SLOTS)], axis=0
        )
        scale = lax.rsqrt(square * (1.0 / 2048.0) + NORM_EPS)
        gate = jnp.minimum(dot(rows, wg[...]) * scale, GATE_LIMIT)
        up = jnp.clip(dot(rows, wu[...]) * scale, -GATE_LIMIT, GATE_LIMIT)
        act = ((up + 1.0) * gate * jax.nn.sigmoid(GATE_SLOPE * gate)).astype(BF16)
        for j in range(N_TP):
            terms = dot(act, wd[:, j * 512 : (j + 1) * 512]).astype(BF16)
            for k in range(4):
                down_send[n, j, k * 3 * NS : (k + 1) * 3 * NS, :] = terms[
                    :, k * 128 : (k + 1) * 128
                ]
        for d in (2, 1, 3):
            peer = lax.rem(tp + d, N_TP)
            copy = pltpu.make_async_remote_copy(
                src_ref=down_send.at[n, peer], dst_ref=down_recv.at[n, d - 1],
                send_sem=d_ssem.at[n, d - 1], recv_sem=d_rsem.at[n, d - 1],
                device_id={"tp": peer}, device_id_type=MESH,
            )
            copy.start()
            d_copies.append(copy)

    def back_copy(r):
        return pltpu.make_async_remote_copy(
            src_ref=send_b.at[r], dst_ref=recv_b.at[me],
            send_sem=b_ssem, recv_sem=b_rsem,
            device_id={"ep": lax.rem(me + r, N_EP)}, device_id_type=MESH,
        )

    for n, group in enumerate(ORDER):
        for copy in d_copies[3 * n : 3 * n + 3]:
            copy.wait_recv()
        total = down_send[n, tp].astype(F32)
        for d in range(N_TP - 1):
            total = total + down_recv[n, d].astype(F32)
        first = group * NS
        send_b[first : first + NS] = (
            dot(unpick[...], total.astype(BF16)).astype(BF16).reshape(NS, 16, 128)
        )

        def send_back(r, carry):
            back_copy(r).start()
            return carry

        lax.fori_loop(max(1, first), first + NS, send_back, 0)
    recv_b[me] = send_b[0]
    some = pl.ds(0, N_EP - 1)
    wait_bytes(recv_b.at[some], b_rsem)
    result = dot(take[...], recv_b[...].reshape(N_EP * 16, 128))
    for k in range(4):
        part = result[k * 32 : (k + 1) * 32] + result[128 + k * 32 : 160 + k * 32]
        out_ref[:, k * 128 : (k + 1) * 128] = (
            residual[:, k * 128 : (k + 1) * 128] + part
        ).astype(BF16)
    for copy in g_copies + d_copies:
        copy.wait_send()
    wait_bytes(send_a.at[some], a_ssem)
    wait_bytes(send_b.at[some], b_ssem)


def tail(mixed, tokens, gain, routes, weight, wout, wg, wu, wd):
    by_choice = routes.T
    vmem = pl.BlockSpec(memory_space=pltpu.VMEM)
    hbm = pl.BlockSpec(memory_space=pl.ANY)
    dma = pltpu.SemaphoreType.DMA
    return pl.pallas_call(
        tail_kernel,
        out_shape=jax.ShapeDtypeStruct((32, 512), BF16),
        in_specs=[vmem] * 7 + [hbm] * 4,
        out_specs=vmem,
        scratch_shapes=[
            pltpu.VMEM((256, 2048), BF16),
            pltpu.VMEM((2048, 256), BF16),
            pltpu.VMEM((2048, 256), BF16),
            pltpu.VMEM((256, 2048), BF16),
            pltpu.VMEM((1024, 256), BF16),
            pltpu.VMEM((256, 1024), BF16),
            pltpu.VMEM((PACKED, 16 * NS), BF16),
            pltpu.VMEM((16 * NS, KEPT), BF16),
            pltpu.VMEM((N_TP, 32, 512), BF16),
            pltpu.VMEM((N_TP - 1, 32, 512), BF16),
            pltpu.VMEM((32, 512), F32),
            pltpu.VMEM((N_EP, 16, 128), BF16),
            pltpu.VMEM((N_EP, 16, 128), BF16),
            pltpu.VMEM((GROUPS, N_TP, PACKED, 128), BF16),
            pltpu.VMEM((GROUPS, N_TP, KEPT, 128), BF16),
            pltpu.VMEM((GROUPS, N_TP - 1, KEPT, 128), BF16),
            pltpu.VMEM((N_EP, 16, 128), BF16),
            pltpu.VMEM((N_EP, 16, 128), BF16),
            dma((4,)),
            dma((N_TP - 1,)),
            dma((N_TP - 1,)),
            dma,
            dma((GROUPS,)),
            dma((GROUPS, N_TP - 1)),
            dma((GROUPS, N_TP - 1)),
            dma((GROUPS, N_TP - 1)),
            dma((GROUPS, N_TP - 1)),
            dma,
            dma,
        ],
        name="tail",
        compiler_params=pltpu.CompilerParams(
            collective_id=1, has_side_effects=True, vmem_limit_bytes=40 * 1024 * 1024
        ),
    )(
        mixed, tokens, gain.reshape(N_TP, 512), routes, by_choice.reshape(1, 128),
        jnp.tile(by_choice, (1, 8)), weight, wout, wg, wu, wd,
    )

def shards(
    tokens,
    previous,
    first_norm_gain,
    token_shift_share,
    receptance_weight,
    key_weight,
    value_weight,
    decay_down_map,
    decay_up_map,
    decay_offset,
    strength_down_map,
    strength_up_map,
    removal_key_scale,
    key_damping,
    self_term_weight,
    head_norm_gain,
    output_weight,
    state,
    second_norm_gain,
    routes,
    chosen_expert_weight,
    expert_gate_weight,
    expert_up_weight,
    expert_down_weight,
):
    present_rows, prior_rows = in_one_piece((tokens, previous), "tp", 1, 0)
    head_columns = receptance_weight.shape[1]
    head_start = lax.axis_index("tp") * head_columns
    decay_own = lax.dynamic_slice_in_dim(decay_up_map, head_start, head_columns, 1)
    alpha_own = lax.dynamic_slice_in_dim(strength_up_map, head_start, head_columns, 1)
    mixed_inputs, new_state = head_combiner(
        present_rows,
        prior_rows,
        first_norm_gain,
        token_shift_share,
        receptance_weight,
        key_weight,
        value_weight,
        decay_down_map,
        decay_own,
        decay_offset,
        strength_down_map,
        alpha_own,
        removal_key_scale,
        key_damping,
        self_term_weight,
        head_norm_gain,
        state,
    )
    layer_out = tail(
        mixed_inputs, tokens, second_norm_gain, routes, chosen_expert_weight,
        output_weight, expert_gate_weight, expert_up_weight, expert_down_weight,
    )
    return (layer_out, new_state)


def solution(mesh):
    in_specs = (
        P("ep", "tp"),
        P("ep", "tp"),
        P(),
        P(),
        P(None, "tp"),
        P(None, "tp"),
        P(None, "tp"),
        P(),
        P(),
        P("tp"),
        P(),
        P(),
        P("tp"),
        P("tp"),
        P("tp", None),
        P("tp"),
        P("tp", None),
        P("ep", "tp", None, None),
        P(),
        P("ep", None),
        P("ep", None),
        P("ep", None, "tp"),
        P("ep", None, "tp"),
        P("ep", "tp", None),
    )
    out_specs = (P("ep", "tp"), P("ep", "tp", None, None))
    return jax.shard_map(shards, mesh=mesh, in_specs=in_specs, out_specs=out_specs, check_vma=False)
```

```python
import jax
import jax.numpy as jnp
from jax import lax
from jax.experimental import pallas as pl
from jax.experimental.pallas import tpu as pltpu
from jax.sharding import PartitionSpec as P

NORM_EPS = 1e-06
GROUP_EPS = 0.00064
KEY_EPS = 1e-06
GATE_LIMIT = 7.0
GATE_SLOPE = 1.702


MESH = pl.DeviceIdType.MESH
N_EP = 64
N_TP = 4
GROUPS = 4
NS = N_EP // GROUPS
ORDER = (0, 3, 1, 2)
SLOTS = 3
KEPT = 4 * SLOTS * NS
PACKED = KEPT + NS
F32 = jnp.float32
BF16 = jnp.bfloat16


def pin(value):
    return pltpu.with_memory_space_constraint(value, pltpu.HBM)


def dot(a, b):
    return jnp.dot(a, b, preferred_element_type=F32)


def iota(shape, dim):
    return lax.broadcasted_iota(jnp.int32, shape, dim)


def third(m):
    return (m * 11) >> 5


def kept_row(m):
    return jnp.where(m == 12, 3, m + third(m))


def gather_kernel(tokens_hbm, previous_hbm, rows_ref, load_sem, send_sem, recv_sem):
    tp = lax.axis_index("tp")
    loads = [
        pltpu.make_async_copy(tokens_hbm, rows_ref.at[tp, pl.ds(0, 32)], load_sem.at[0]),
        pltpu.make_async_copy(previous_hbm, rows_ref.at[tp, pl.ds(32, 32)], load_sem.at[1]),
    ]
    for load in loads:
        load.start()
    barrier = pltpu.get_barrier_semaphore()
    for d in range(1, N_TP):
        pl.semaphore_signal(
            barrier, inc=1, device_id={"tp": lax.rem(tp + d, N_TP)}, device_id_type=MESH
        )
    for load in loads:
        load.wait()
    pl.semaphore_wait(barrier, N_TP - 1)
    copies = []
    for d in (2, 1, 3):
        copy = pltpu.make_async_remote_copy(
            src_ref=rows_ref.at[tp], dst_ref=rows_ref.at[tp],
            send_sem=send_sem.at[d - 1], recv_sem=recv_sem.at[d - 1],
            device_id={"tp": lax.rem(tp + d, N_TP)}, device_id_type=MESH,
        )
        copy.start()
        copies.append(copy)
    for copy in copies:
        copy.wait()


def gather(tokens, previous):
    hbm = pl.BlockSpec(memory_space=pltpu.HBM)
    dma = pltpu.SemaphoreType.DMA
    return pl.pallas_call(
        gather_kernel,
        out_shape=jax.ShapeDtypeStruct((N_TP, 64, 512), BF16),
        in_specs=[hbm, hbm],
        out_specs=pl.BlockSpec(memory_space=pltpu.VMEM),
        scratch_shapes=[dma((2,)), dma((N_TP - 1,)), dma((N_TP - 1,))],
        name="gather",
        compiler_params=pltpu.CompilerParams(
            collective_id=0, has_side_effects=True, vmem_limit_bytes=4 * 1024 * 1024
        ),
    )(tokens, previous)


def head_sums(values):
    same = iota((256, 256), 0) // 64 == iota((256, 256), 1) // 64
    return jnp.dot(
        values, same.astype(F32), preferred_element_type=F32, precision=lax.Precision.HIGHEST
    )


def column(row):
    eye = iota((32, 32), 0) == iota((32, 32), 1)
    return jnp.sum(jnp.where(eye, row, jnp.zeros_like(row)), axis=1, keepdims=True)


def layer_kernel(
    rows_ref,
    gain_one_hbm, share_hbm, offset_hbm, key_scale_hbm, damping_hbm, self_hbm, head_gain_hbm,
    gain_hbm, routes_hbm, weight_hbm,
    wr_hbm, wk_hbm, wv_hbm, dd_hbm, du_hbm, sd_hbm, su_hbm, state_hbm,
    wout_hbm, wg_hbm, wu_hbm, wd_hbm,
    out_ref, state,
    gain_one_ref, share_ref, offset_ref, key_scale_ref, damping_ref, self_pair, head_gain_ref,
    gain_ref, routes_ref, weight_ref, self_ref, routes_row_ref, routes_tiled_ref,
    wr, wk, wv, dd, du, sd, su, along_scr, query_scr, rows_scr,
    wout, wg, wu, wd, place, take, pick, unpick,
    rs_send, rs_recv, residual, send_a, recv_a, gathered, down_send, down_recv, send_b, recv_b,
    w_sem, h_sem, p_sem, rs_ssem, rs_rsem, a_ssem, a_rsem, g_ssem, g_rsem, d_ssem, d_rsem, b_ssem, b_rsem,
):
    me = lax.axis_index("ep")
    tp = lax.axis_index("tp")
    own = pl.ds(pl.multiple_of(tp * 256, 256), 256)
    small_loads = [
        pltpu.make_async_copy(source, target, p_sem.at[n])
        for n, (source, target) in enumerate(
            [
                (gain_one_hbm, gain_one_ref), (share_hbm, share_ref), (offset_hbm, offset_ref),
                (key_scale_hbm, key_scale_ref), (damping_hbm, damping_ref), (self_hbm, self_pair),
                (head_gain_hbm, head_gain_ref),
                (gain_hbm.at[:, pl.ds(pl.multiple_of(tp * 512, 512), 512)], gain_ref),
                (routes_hbm, routes_ref), (weight_hbm, weight_ref),
            ]
        )
    ]
    for load in small_loads:
        load.start()
    head_loads = [
        pltpu.make_async_copy(source, target, h_sem.at[n])
        for n, (source, target) in enumerate(
            [
                (dd_hbm, dd), (sd_hbm, sd), (wk_hbm, wk), (wr_hbm, wr), (wv_hbm, wv),
                (du_hbm.at[:, own], du), (su_hbm.at[:, own], su), (state_hbm, state),
            ]
        )
    ]
    for load in head_loads:
        load.start()
    loads = [
        pltpu.make_async_copy(wout_hbm, wout, w_sem.at[0]),
        pltpu.make_async_copy(wg_hbm.at[0], wg, w_sem.at[1]),
        pltpu.make_async_copy(wu_hbm.at[0], wu, w_sem.at[2]),
        pltpu.make_async_copy(wd_hbm.at[0], wd, w_sem.at[3]),
    ]
    for load in loads:
        load.start()
    barrier = pltpu.get_barrier_semaphore()
    for d in range(1, N_TP):
        pl.semaphore_signal(
            barrier, inc=1, device_id={"tp": lax.rem(tp + d, N_TP)}, device_id_type=MESH
        )

    def greet(d, carry):
        pl.semaphore_signal(
            barrier, inc=1, device_id={"ep": lax.rem(me + d, N_EP)}, device_id_type=MESH
        )
        return carry

    lax.fori_loop(1, N_EP, greet, 0)

    for load in small_loads:
        load.wait()
    for h in range(4):
        self_ref[:, h * 64 : (h + 1) * 64] = self_pair[h : h + 1, :]
    for c in range(4):
        routes_row_ref[:, c * 32 : (c + 1) * 32] = routes_ref[c : c + 1, :]
    for b in range(8):
        routes_tiled_ref[:, b * 32 : (b + 1) * 32] = routes_ref[...]
    square = jnp.zeros((32, 1), F32)
    for t in range(N_TP):
        part = rows_ref[t, 0:32, :].astype(F32)
        square = square + jnp.sum(part * part, axis=1, keepdims=True)
    scale = lax.rsqrt(square * (1.0 / 2048.0) + NORM_EPS)
    sums = [None] * 5
    for t in range(N_TP):
        span = slice(t * 512, (t + 1) * 512)
        normed = rows_ref[t, 0:32, :].astype(F32) * scale * gain_one_ref[:, span]
        change = rows_ref[t, 32:64, :].astype(F32) - normed
        for n, (m, weight) in enumerate([(3, dd), (4, sd), (1, wk), (0, wr), (2, wv)]):
            if t == 0:
                head_loads[n].wait()
            shifted = (normed + change * share_ref[m : m + 1, span]).astype(BF16)
            term = dot(shifted, weight[span, :])
            sums[n] = term if t == 0 else sums[n] + term
    low, strength_low, key, receptance, value = sums
    head_loads[5].wait()
    decay = dot(jnp.tanh(low).astype(BF16), du[...]) + offset_ref[...]
    decay = jnp.exp(jax.nn.sigmoid(decay) * -(2.718281828459045 ** -0.5))
    head_loads[6].wait()
    alpha = jax.nn.sigmoid(dot(strength_low.astype(BF16), su[...]))
    removal = key * key_scale_ref[...]
    removal = removal * lax.rsqrt(head_sums(removal * removal) + KEY_EPS)
    blended = key * (1.0 + (alpha - 1.0) * damping_ref[...])
    strong = removal * alpha
    query = decay * receptance
    both = head_sums(
        jnp.concatenate(
            [strong * receptance, blended * receptance, blended * receptance * self_ref[...]], axis=0
        )
    )
    head_loads[7].wait()
    for h in range(4):
        lanes = slice(h * 64, (h + 1) * 64)
        asked = jnp.concatenate([removal[:, lanes], query[:, lanes]], axis=0).astype(BF16)
        for q in range(8):
            held = state[4 * q : 4 * q + 4, h].reshape(256, 64).astype(BF16)
            answer = lax.dot_general(
                asked, held, (((1,), (1,)), ((), ())), preferred_element_type=F32
            )
            for j in range(4):
                s = 4 * q + j
                span = slice(j * 64, (j + 1) * 64)
                along_scr[s : s + 1, lanes] = answer[s : s + 1, span]
                query_scr[s : s + 1, lanes] = answer[32 + s : 33 + s, span]
    along = along_scr[...]
    readout = query_scr[...] - along * both[0:32] + value * both[32:64]
    centred = readout - head_sums(readout) * (1.0 / 64.0)
    spread = head_sums(centred * centred) * (1.0 / 64.0)
    mixed = centred * lax.rsqrt(spread + GROUP_EPS) * head_gain_ref[...] + both[64:96] * value
    mixed = mixed.astype(BF16)
    for n, values in enumerate((-along, value, strong, blended, decay)):
        for h in range(4):
            rows_scr[n, h] = values[:, h * 64 : (h + 1) * 64]

    loads[0].wait()
    for j in range(N_TP):
        rs_send[j] = dot(mixed, wout[:, j * 512 : (j + 1) * 512]).astype(BF16)
    pl.semaphore_wait(barrier, N_EP - 1 + N_TP - 1)
    rs_copies = []
    for d in (2, 1, 3):
        peer = lax.rem(tp + d, N_TP)
        copy = pltpu.make_async_remote_copy(
            src_ref=rs_send.at[peer], dst_ref=rs_recv.at[d - 1],
            send_sem=rs_ssem.at[d - 1], recv_sem=rs_rsem.at[d - 1],
            device_id={"tp": peer}, device_id_type=MESH,
        )
        copy.start()
        rs_copies.append(copy)

    lane = iota((1, 256), 1)
    block, seq = lane // 32, lane % 32
    source = iota((32, 256), 0)
    routed = [column(routes_ref[c : c + 1, :]) for c in range(4)]
    targets = []
    for c in range(4):
        mine = routes_tiled_ref[c : c + 1, :]
        rank = jnp.zeros((1, 256), jnp.int32)
        for other in range(c + 1):
            same = routed[other] == mine
            if other == c:
                same = same & (source < seq)
            rank = rank + jnp.sum(same.astype(jnp.int32), axis=0, keepdims=True)
        row = jnp.where(block < 4, block * 4 + rank, jnp.where(rank == block - 4, 3, -4096))
        targets.append(mine * 16 + row)

    def fill_place(i, carry):
        at = pl.multiple_of(i * 128, 128)
        row = iota((128, 256), 0) + at
        hit = row == targets[0]
        for c in range(1, 4):
            hit = hit | (row == targets[c])
        place[pl.ds(at, 128), :] = hit.astype(F32).astype(BF16)
        return carry

    lax.fori_loop(0, 8, fill_place, 0)

    piece, tile_row = iota((PACKED, 16 * NS), 0), iota((PACKED, 16 * NS), 1)
    pick[...] = (tile_row == (piece % NS) * 16 + kept_row(piece // NS)).astype(F32).astype(BF16)
    tile_row, piece = iota((16 * NS, KEPT), 0), iota((16 * NS, KEPT), 1)
    unpick[...] = (tile_row == (piece % NS) * 16 + kept_row(piece // NS)).astype(F32).astype(BF16)

    for copy in rs_copies:
        copy.wait()
    total = rows_ref[tp, 0:32, :].astype(F32) + rs_send[tp].astype(F32)
    for d in range(N_TP - 1):
        total = total + rs_recv[d].astype(F32)
    residual[...] = total
    square = jnp.sum(total * total, axis=1, keepdims=True)
    high = square.astype(BF16).astype(F32)
    low = square - high
    scaled = total * gain_ref[...]
    stack = [scaled[:, k * 128 : (k + 1) * 128] for k in range(4)]
    sum_lane = iota((32, 128), 1)
    for j in range(SLOTS):
        stack.append(jnp.where(sum_lane == j, high, jnp.where(sum_lane == 3 + j, low, 0.0)))
    stack.append(jnp.zeros((32, 128), F32))
    stack = jnp.concatenate(stack, axis=0).astype(BF16)
    send_a[...] = dot(place[...], stack).astype(BF16).reshape(N_EP, 16, 128)

    def out_copy(r, group):
        peer = lax.rem(me + N_EP - r, N_EP)
        return pltpu.make_async_remote_copy(
            src_ref=send_a.at[peer], dst_ref=recv_a.at[r],
            send_sem=a_ssem, recv_sem=a_rsem.at[group],
            device_id={"ep": peer}, device_id_type=MESH,
        )

    for group in ORDER:

        def send_out(r, carry, group=group):
            out_copy(r, group).start()
            return carry

        lax.fori_loop(max(1, group * NS), (group + 1) * NS, send_out, 0)
    recv_a[0] = send_a[me]

    seq_col = iota((32, 128), 0)
    earlier = iota((32, 128), 1)
    columns = []
    for c in range(4):
        mine = routed[c]
        same = (routes_row_ref[...] == mine) & (earlier < c * 32 + seq_col)
        columns.append(mine * 16 + jnp.sum(same.astype(jnp.int32), axis=1, keepdims=True))
    weights = [column(weight_ref[c : c + 1, :]) for c in range(4)]
    for k in range(4):
        for j in range(8):
            at = iota((32, 128), 1) + (j * 128 - k * 4)
            share = jnp.zeros((32, 128), F32)
            for c in range(4):
                share = jnp.where(at == columns[c], weights[c], share)
            upper = share.astype(BF16)
            take[k * 32 : (k + 1) * 32, j * 128 : (j + 1) * 128] = upper
            take[128 + k * 32 : 160 + k * 32, j * 128 : (j + 1) * 128] = (
                share - upper.astype(F32)
            ).astype(BF16)

    upper_row = iota((8, 64), 0)

    def renew(s, carry):
        for h in range(4):
            minus, given, strong_row, blended_row, decay_row = [
                rows_scr[n, h, pl.ds(s, 1), :] for n in range(5)
            ]
            zero = jnp.zeros((8, 64), F32)
            left = jnp.where(upper_row == 0, minus, jnp.where(upper_row == 1, given, zero))
            right = jnp.where(upper_row == 0, strong_row, jnp.where(upper_row == 1, blended_row, zero))
            change = lax.dot_general(
                left, right, (((0,), (0,)), ((), ())),
                preferred_element_type=F32, precision=lax.Precision.HIGHEST,
            )
            state[s, h] = state[s, h] * decay_row + change
        return carry

    lax.fori_loop(0, 32, renew, 0)

    def wait_bytes(ref, sem):
        pltpu.make_async_copy(ref, ref, sem).wait()

    g_copies = []
    for n, group in enumerate(ORDER):
        first = group * NS
        count = NS - 1 if group == 0 else NS
        wait_bytes(recv_a.at[pl.ds(first, count)], a_rsem.at[group])
        tiles = recv_a[first : first + NS].reshape(NS * 16, 128)
        gathered[n, tp] = dot(pick[...], tiles).astype(BF16)
        for d in (2, 1, 3):
            copy = pltpu.make_async_remote_copy(
                src_ref=gathered.at[n, tp], dst_ref=gathered.at[n, tp],
                send_sem=g_ssem.at[n, d - 1], recv_sem=g_rsem.at[n, d - 1],
                device_id={"tp": lax.rem(tp + d, N_TP)}, device_id_type=MESH,
            )
            copy.start()
            g_copies.append(copy)
    for load in loads[1:]:
        load.wait()
    d_copies = []
    for n, group in enumerate(ORDER):
        for copy in g_copies[3 * n : 3 * n + 3]:
            copy.wait_recv()
        rows, sums = [], None
        for t in range(N_TP):
            for k in range(4):
                rows.append(gathered[n, t, k * 3 * NS : (k + 1) * 3 * NS, :])
            part = gathered[n, t, KEPT:PACKED, :].astype(F32)
            sums = part if sums is None else sums + part
        rows = jnp.concatenate(rows, axis=1)
        square = jnp.concatenate(
            [sums[:, j : j + 1] + sums[:, 3 + j : 4 + j] for j in range(SLOTS)], axis=0
        )
        scale = lax.rsqrt(square * (1.0 / 2048.0) + NORM_EPS)
        gate = jnp.minimum(dot(rows, wg[...]) * scale, GATE_LIMIT)
        up = jnp.clip(dot(rows, wu[...]) * scale, -GATE_LIMIT, GATE_LIMIT)
        act = ((up + 1.0) * gate * jax.nn.sigmoid(GATE_SLOPE * gate)).astype(BF16)
        for j in range(N_TP):
            terms = dot(act, wd[:, j * 512 : (j + 1) * 512]).astype(BF16)
            for k in range(4):
                down_send[n, j, k * 3 * NS : (k + 1) * 3 * NS, :] = terms[
                    :, k * 128 : (k + 1) * 128
                ]
        for d in (2, 1, 3):
            peer = lax.rem(tp + d, N_TP)
            copy = pltpu.make_async_remote_copy(
                src_ref=down_send.at[n, peer], dst_ref=down_recv.at[n, d - 1],
                send_sem=d_ssem.at[n, d - 1], recv_sem=d_rsem.at[n, d - 1],
                device_id={"tp": peer}, device_id_type=MESH,
            )
            copy.start()
            d_copies.append(copy)

    def back_copy(r):
        return pltpu.make_async_remote_copy(
            src_ref=send_b.at[r], dst_ref=recv_b.at[me],
            send_sem=b_ssem, recv_sem=b_rsem,
            device_id={"ep": lax.rem(me + r, N_EP)}, device_id_type=MESH,
        )

    for n, group in enumerate(ORDER):
        for copy in d_copies[3 * n : 3 * n + 3]:
            copy.wait_recv()
        total = down_send[n, tp].astype(F32)
        for d in range(N_TP - 1):
            total = total + down_recv[n, d].astype(F32)
        first = group * NS
        send_b[first : first + NS] = (
            dot(unpick[...], total.astype(BF16)).astype(BF16).reshape(NS, 16, 128)
        )

        def send_back(r, carry):
            back_copy(r).start()
            return carry

        lax.fori_loop(max(1, first), first + NS, send_back, 0)
    recv_b[me] = send_b[0]
    some = pl.ds(0, N_EP - 1)
    wait_bytes(recv_b.at[some], b_rsem)
    result = dot(take[...], recv_b[...].reshape(N_EP * 16, 128))
    for k in range(4):
        part = result[k * 32 : (k + 1) * 32] + result[128 + k * 32 : 160 + k * 32]
        out_ref[:, k * 128 : (k + 1) * 128] = (
            residual[:, k * 128 : (k + 1) * 128] + part
        ).astype(BF16)
    for copy in g_copies + d_copies:
        copy.wait_send()
    wait_bytes(send_a.at[some], a_ssem)
    wait_bytes(send_b.at[some], b_ssem)


def layer(
    rows, gain_one, share, offset, key_scale, damping, self_weight, head_gain, gain, routes, weight,
    wr, wk, wv, dd, du, sd, su, state, wout, wg, wu, wd,
):
    vmem = pl.BlockSpec(memory_space=pltpu.VMEM)
    hbm = pl.BlockSpec(memory_space=pltpu.HBM)
    dma = pltpu.SemaphoreType.DMA
    return pl.pallas_call(
        layer_kernel,
        out_shape=(
            pltpu.VMEM((32, 512), BF16),
            pltpu.VMEM((32, 4, 64, 64), F32),
        ),
        in_specs=[vmem] + [hbm] * 22,
        out_specs=(vmem, vmem),
        scratch_shapes=[
            pltpu.VMEM((1, 2048), F32),
            pltpu.VMEM((5, 2048), F32),
            pltpu.VMEM((1, 256), F32),
            pltpu.VMEM((1, 256), F32),
            pltpu.VMEM((1, 256), F32),
            pltpu.VMEM((4, 64), F32),
            pltpu.VMEM((1, 256), F32),
            pltpu.VMEM((1, 512), F32),
            pltpu.VMEM((4, 32), jnp.int32),
            pltpu.VMEM((4, 32), F32),
            pltpu.VMEM((1, 256), F32),
            pltpu.VMEM((1, 128), jnp.int32),
            pltpu.VMEM((4, 256), jnp.int32),
            pltpu.VMEM((2048, 256), BF16),
            pltpu.VMEM((2048, 256), BF16),
            pltpu.VMEM((2048, 256), BF16),
            pltpu.VMEM((2048, 128), BF16),
            pltpu.VMEM((128, 256), BF16),
            pltpu.VMEM((2048, 128), BF16),
            pltpu.VMEM((128, 256), BF16),
            pltpu.VMEM((32, 256), F32),
            pltpu.VMEM((32, 256), F32),
            pltpu.VMEM((5, 4, 32, 64), F32),
            pltpu.VMEM((256, 2048), BF16),
            pltpu.VMEM((2048, 256), BF16),
            pltpu.VMEM((2048, 256), BF16),
            pltpu.VMEM((256, 2048), BF16),
            pltpu.VMEM((1024, 256), BF16),
            pltpu.VMEM((256, 1024), BF16),
            pltpu.VMEM((PACKED, 16 * NS), BF16),
            pltpu.VMEM((16 * NS, KEPT), BF16),
            pltpu.VMEM((N_TP, 32, 512), BF16),
            pltpu.VMEM((N_TP - 1, 32, 512), BF16),
            pltpu.VMEM((32, 512), F32),
            pltpu.VMEM((N_EP, 16, 128), BF16),
            pltpu.VMEM((N_EP, 16, 128), BF16),
            pltpu.VMEM((GROUPS, N_TP, PACKED, 128), BF16),
            pltpu.VMEM((GROUPS, N_TP, KEPT, 128), BF16),
            pltpu.VMEM((GROUPS, N_TP - 1, KEPT, 128), BF16),
            pltpu.VMEM((N_EP, 16, 128), BF16),
            pltpu.VMEM((N_EP, 16, 128), BF16),
            dma((4,)),
            dma((8,)),
            dma((10,)),
            dma((N_TP - 1,)),
            dma((N_TP - 1,)),
            dma,
            dma((GROUPS,)),
            dma((GROUPS, N_TP - 1)),
            dma((GROUPS, N_TP - 1)),
            dma((GROUPS, N_TP - 1)),
            dma((GROUPS, N_TP - 1)),
            dma,
            dma,
        ],
        name="layer",
        compiler_params=pltpu.CompilerParams(
            collective_id=1, has_side_effects=True, vmem_limit_bytes=48 * 1024 * 1024
        ),
    )(
        rows, *map(pin, (gain_one.reshape(1, 2048), share, offset.reshape(1, 256), key_scale.reshape(1, 256),
        damping.reshape(1, 256), self_weight, head_gain.reshape(1, 256),
        gain.reshape(1, 2048), routes.T, weight.T, wr, wk, wv, dd, du, sd, su, state, wout, wg, wu, wd))
    )


def shards(
    tokens,
    previous,
    first_norm_gain,
    token_shift_share,
    receptance_weight,
    key_weight,
    value_weight,
    decay_down_map,
    decay_up_map,
    decay_offset,
    strength_down_map,
    strength_up_map,
    removal_key_scale,
    key_damping,
    self_term_weight,
    head_norm_gain,
    output_weight,
    state,
    second_norm_gain,
    routes,
    chosen_expert_weight,
    expert_gate_weight,
    expert_up_weight,
    expert_down_weight,
):
    return layer(
        gather(pin(tokens), pin(previous)), first_norm_gain, token_shift_share, decay_offset,
        removal_key_scale, key_damping, self_term_weight, head_norm_gain, second_norm_gain,
        routes, chosen_expert_weight, receptance_weight, key_weight, value_weight,
        decay_down_map, decay_up_map, strength_down_map, strength_up_map, state,
        output_weight, expert_gate_weight, expert_up_weight, expert_down_weight,
    )


def solution(mesh):
    in_specs = (
        P("ep", "tp"),
        P("ep", "tp"),
        P(),
        P(),
        P(None, "tp"),
        P(None, "tp"),
        P(None, "tp"),
        P(),
        P(),
        P("tp"),
        P(),
        P(),
        P("tp"),
        P("tp"),
        P("tp", None),
        P("tp"),
        P("tp", None),
        P("ep", "tp", None, None),
        P(),
        P("ep", None),
        P("ep", None),
        P("ep", None, "tp"),
        P("ep", None, "tp"),
        P("ep", "tp", None),
    )
    out_specs = (P("ep", "tp"), P("ep", "tp", None, None))
    return jax.shard_map(shards, mesh=mesh, in_specs=in_specs, out_specs=out_specs, check_vma=False)
```

```python
import jax
import jax.numpy as jnp
from jax import lax
from jax.experimental import pallas as pl
from jax.experimental.pallas import tpu as pltpu
from jax.sharding import PartitionSpec as P

NORM_EPS = 1e-06
GROUP_EPS = 0.00064
KEY_EPS = 1e-06
GATE_LIMIT = 7.0
GATE_SLOPE = 1.702


MESH = pl.DeviceIdType.MESH
N_EP = 64
N_TP = 4
GROUPS = 4
NS = N_EP // GROUPS
ORDER = (0, 3, 1, 2)
EARLY = 15
SLOTS = 3
KEPT = 4 * SLOTS * NS
PACKED = KEPT + NS
F32 = jnp.float32
BF16 = jnp.bfloat16


def pin(value):
    return pltpu.with_memory_space_constraint(value, pltpu.HBM)


def dot(a, b):
    return jnp.dot(a, b, preferred_element_type=F32)


def iota(shape, dim):
    return lax.broadcasted_iota(jnp.int32, shape, dim)


def third(m):
    return (m * 11) >> 5


def kept_row(m):
    return jnp.where(m == 12, 3, m + third(m))


def gather_kernel(
    tokens_hbm, previous_hbm, *refs,
):
    kept = len(PARTS)
    sources, (rows_ref, *targets) = refs[:kept], refs[kept : 2 * kept + 1]
    load_sem, part_sem, send_sem, recv_sem = refs[2 * kept + 1 :]
    tp = lax.axis_index("tp")
    loads = [
        pltpu.make_async_copy(tokens_hbm, rows_ref.at[tp, pl.ds(0, 32)], load_sem.at[0]),
        pltpu.make_async_copy(previous_hbm, rows_ref.at[tp, pl.ds(32, 32)], load_sem.at[1]),
    ]
    for load in loads:
        load.start()
    barrier = pltpu.get_barrier_semaphore()
    for d in range(1, N_TP):
        pl.semaphore_signal(
            barrier, inc=1, device_id={"tp": lax.rem(tp + d, N_TP)}, device_id_type=MESH
        )
    part_loads = []
    for n, (source, target, (shape, dtype, cut)) in enumerate(zip(sources, targets, PARTS)):
        if cut:
            source = source.at[:, pl.ds(pl.multiple_of(tp * cut, cut), cut)]
        load = pltpu.make_async_copy(source, target, part_sem.at[n])
        load.start()
        part_loads.append(load)
    for load in loads:
        load.wait()
    pl.semaphore_wait(barrier, N_TP - 1)
    copies = []
    for d in (2, 1, 3):
        copy = pltpu.make_async_remote_copy(
            src_ref=rows_ref.at[tp], dst_ref=rows_ref.at[tp],
            send_sem=send_sem.at[d - 1], recv_sem=recv_sem.at[d - 1],
            device_id={"tp": lax.rem(tp + d, N_TP)}, device_id_type=MESH,
        )
        copy.start()
        copies.append(copy)
    for load in part_loads:
        load.wait()
    for copy in copies:
        copy.wait()


PARTS = [
    ((1, 2048), F32, 0),
    ((5, 2048), F32, 0),
    ((1, 256), F32, 0),
    ((1, 256), F32, 0),
    ((1, 256), F32, 0),
    ((4, 64), F32, 0),
    ((1, 256), F32, 0),
    ((1, 512), F32, 512),
    ((4, 32), jnp.int32, 0),
    ((4, 32), F32, 0),
    ((2048, 128), BF16, 0),
    ((2048, 128), BF16, 0),
    ((2048, 256), BF16, 0),
    ((2048, 256), BF16, 0),
    ((2048, 256), BF16, 0),
    ((128, 256), BF16, 256),
    ((128, 256), BF16, 256),
    ((32, 4, 64, 64), F32, 0),
    ((256, 2048), BF16, 0),
]


def gather(tokens, previous, parts):
    hbm = pl.BlockSpec(memory_space=pltpu.HBM)
    vmem = pl.BlockSpec(memory_space=pltpu.VMEM)
    dma = pltpu.SemaphoreType.DMA
    return pl.pallas_call(
        gather_kernel,
        out_shape=[pltpu.VMEM((N_TP, 64, 512), BF16)]
        + [pltpu.VMEM(shape, dtype) for shape, dtype, _ in PARTS],
        in_specs=[hbm] * (2 + len(PARTS)),
        out_specs=[vmem] * (1 + len(PARTS)),
        scratch_shapes=[dma((2,)), dma((len(PARTS),)), dma((N_TP - 1,)), dma((N_TP - 1,))],
        name="gather",
        compiler_params=pltpu.CompilerParams(
            collective_id=0, has_side_effects=True, vmem_limit_bytes=16 * 1024 * 1024
        ),
    )(pin(tokens), pin(previous), *map(pin, parts))


def head_sums(values):
    same = iota((256, 256), 0) // 64 == iota((256, 256), 1) // 64
    return jnp.dot(
        values, same.astype(F32), preferred_element_type=F32, precision=lax.Precision.HIGHEST
    )


def column(row):
    eye = iota((32, 32), 0) == iota((32, 32), 1)
    return jnp.sum(jnp.where(eye, row, jnp.zeros_like(row)), axis=1, keepdims=True)


def layer_kernel(
    rows_ref,
    gain_one_ref, share_ref, offset_ref, key_scale_ref, damping_ref, self_pair, head_gain_ref,
    gain_ref, routes_ref, weight_ref, dd, sd, wk, wr, wv, du, su, old_state, wout,
    wg_hbm, wu_hbm, wd_hbm,
    out_ref, state,
    self_ref, routes_row_ref, routes_tiled_ref, along_scr, query_scr, rows_scr,
    wg, wu, wd, place, take, pick, unpick,
    rs_send, rs_recv, residual, send_a, recv_a, gathered, down_send, down_recv, send_b, recv_b,
    w_sem, rs_ssem, rs_rsem, a_ssem, a_rsem, g_ssem, g_rsem, d_ssem, d_rsem, b_ssem, b_rsem,
):
    me = lax.axis_index("ep")
    tp = lax.axis_index("tp")
    loads = [
        pltpu.make_async_copy(wg_hbm.at[0], wg, w_sem.at[0]),
        pltpu.make_async_copy(wu_hbm.at[0], wu, w_sem.at[1]),
        pltpu.make_async_copy(wd_hbm.at[0], wd, w_sem.at[2]),
    ]
    for load in loads:
        load.start()
    barrier = pltpu.get_barrier_semaphore()
    for d in range(1, N_TP):
        pl.semaphore_signal(
            barrier, inc=1, device_id={"tp": lax.rem(tp + d, N_TP)}, device_id_type=MESH
        )

    def greet(d, carry):
        pl.semaphore_signal(
            barrier, inc=1, device_id={"ep": lax.rem(me + d, N_EP)}, device_id_type=MESH
        )
        return carry

    lax.fori_loop(1, N_EP, greet, 0)

    for h in range(4):
        self_ref[:, h * 64 : (h + 1) * 64] = self_pair[h : h + 1, :]
    for c in range(4):
        routes_row_ref[:, c * 32 : (c + 1) * 32] = routes_ref[c : c + 1, :]
    for b in range(8):
        routes_tiled_ref[:, b * 32 : (b + 1) * 32] = routes_ref[...]
    square = jnp.zeros((32, 1), F32)
    for t in range(N_TP):
        part = rows_ref[t, 0:32, :].astype(F32)
        square = square + jnp.sum(part * part, axis=1, keepdims=True)
    scale = lax.rsqrt(square * (1.0 / 2048.0) + NORM_EPS)
    sums = [None] * 5
    for t in range(N_TP):
        span = slice(t * 512, (t + 1) * 512)
        normed = rows_ref[t, 0:32, :].astype(F32) * scale * gain_one_ref[:, span]
        change = rows_ref[t, 32:64, :].astype(F32) - normed
        for n, (m, weight) in enumerate([(3, dd), (4, sd), (1, wk), (0, wr), (2, wv)]):
            shifted = (normed + change * share_ref[m : m + 1, span]).astype(BF16)
            term = dot(shifted, weight[span, :])
            sums[n] = term if t == 0 else sums[n] + term
    low, strength_low, key, receptance, value = sums
    decay = dot(jnp.tanh(low).astype(BF16), du[...]) + offset_ref[...]
    decay = jnp.exp(jax.nn.sigmoid(decay) * -(2.718281828459045 ** -0.5))
    alpha = jax.nn.sigmoid(dot(strength_low.astype(BF16), su[...]))
    removal = key * key_scale_ref[...]
    removal = removal * lax.rsqrt(head_sums(removal * removal) + KEY_EPS)
    blended = key * (1.0 + (alpha - 1.0) * damping_ref[...])
    strong = removal * alpha
    query = decay * receptance
    both = head_sums(
        jnp.concatenate(
            [strong * receptance, blended * receptance, blended * receptance * self_ref[...]], axis=0
        )
    )
    for h in range(4):
        lanes = slice(h * 64, (h + 1) * 64)
        asked = jnp.concatenate([removal[:, lanes], query[:, lanes]], axis=0).astype(BF16)
        for q in range(8):
            held = old_state[4 * q : 4 * q + 4, h].reshape(256, 64).astype(BF16)
            answer = lax.dot_general(
                asked, held, (((1,), (1,)), ((), ())), preferred_element_type=F32
            )
            for j in range(4):
                s = 4 * q + j
                span = slice(j * 64, (j + 1) * 64)
                along_scr[s : s + 1, lanes] = answer[s : s + 1, span]
                query_scr[s : s + 1, lanes] = answer[32 + s : 33 + s, span]
    along = along_scr[...]
    readout = query_scr[...] - along * both[0:32] + value * both[32:64]
    centred = readout - head_sums(readout) * (1.0 / 64.0)
    spread = head_sums(centred * centred) * (1.0 / 64.0)
    mixed = centred * lax.rsqrt(spread + GROUP_EPS) * head_gain_ref[...] + both[64:96] * value
    mixed = mixed.astype(BF16)
    for n, values in enumerate((-along, value, strong, blended, decay)):
        for h in range(4):
            rows_scr[n, h] = values[:, h * 64 : (h + 1) * 64]

    for j in range(N_TP):
        rs_send[j] = dot(mixed, wout[:, j * 512 : (j + 1) * 512]).astype(BF16)
    pl.semaphore_wait(barrier, N_EP - 1 + N_TP - 1)
    rs_copies = []
    for d in (2, 1, 3):
        peer = lax.rem(tp + d, N_TP)
        copy = pltpu.make_async_remote_copy(
            src_ref=rs_send.at[peer], dst_ref=rs_recv.at[d - 1],
            send_sem=rs_ssem.at[d - 1], recv_sem=rs_rsem.at[d - 1],
            device_id={"tp": peer}, device_id_type=MESH,
        )
        copy.start()
        rs_copies.append(copy)

    lane = iota((1, 256), 1)
    block, seq = lane // 32, lane % 32
    source = iota((32, 256), 0)
    routed = [column(routes_ref[c : c + 1, :]) for c in range(4)]
    targets = []
    for c in range(4):
        mine = routes_tiled_ref[c : c + 1, :]
        rank = jnp.zeros((1, 256), jnp.int32)
        for other in range(c + 1):
            same = routed[other] == mine
            if other == c:
                same = same & (source < seq)
            rank = rank + jnp.sum(same.astype(jnp.int32), axis=0, keepdims=True)
        row = jnp.where(block < 4, block * 4 + rank, jnp.where(rank == block - 4, 3, -4096))
        targets.append(mine * 16 + row)

    def fill_place(i, carry):
        at = pl.multiple_of(i * 128, 128)
        row = iota((128, 256), 0) + at
        hit = row == targets[0]
        for c in range(1, 4):
            hit = hit | (row == targets[c])
        place[pl.ds(at, 128), :] = hit.astype(F32).astype(BF16)
        return carry

    lax.fori_loop(0, 8, fill_place, 0)

    piece, tile_row = iota((PACKED, 16 * NS), 0), iota((PACKED, 16 * NS), 1)
    pick[...] = (tile_row == (piece % NS) * 16 + kept_row(piece // NS)).astype(F32).astype(BF16)
    tile_row, piece = iota((16 * NS, KEPT), 0), iota((16 * NS, KEPT), 1)
    unpick[...] = (tile_row == (piece % NS) * 16 + kept_row(piece // NS)).astype(F32).astype(BF16)

    for copy in rs_copies:
        copy.wait()
    total = rows_ref[tp, 0:32, :].astype(F32) + rs_send[tp].astype(F32)
    for d in range(N_TP - 1):
        total = total + rs_recv[d].astype(F32)
    residual[...] = total
    square = jnp.sum(total * total, axis=1, keepdims=True)
    high = square.astype(BF16).astype(F32)
    low = square - high
    scaled = total * gain_ref[...]
    stack = [scaled[:, k * 128 : (k + 1) * 128] for k in range(4)]
    sum_lane = iota((32, 128), 1)
    for j in range(SLOTS):
        stack.append(jnp.where(sum_lane == j, high, jnp.where(sum_lane == 3 + j, low, 0.0)))
    stack.append(jnp.zeros((32, 128), F32))
    stack = jnp.concatenate(stack, axis=0).astype(BF16)
    send_a[...] = dot(place[...], stack).astype(BF16).reshape(N_EP, 16, 128)

    def out_copy(r, group):
        peer = lax.rem(me + N_EP - r, N_EP)
        return pltpu.make_async_remote_copy(
            src_ref=send_a.at[peer], dst_ref=recv_a.at[r],
            send_sem=a_ssem, recv_sem=a_rsem.at[group],
            device_id={"ep": peer}, device_id_type=MESH,
        )

    for group in ORDER:

        def send_out(r, carry, group=group):
            out_copy(r, group).start()
            return carry

        lax.fori_loop(max(1, group * NS), (group + 1) * NS, send_out, 0)
    recv_a[0] = send_a[me]

    seq_col = iota((32, 128), 0)
    earlier = iota((32, 128), 1)
    columns = []
    for c in range(4):
        mine = routed[c]
        same = (routes_row_ref[...] == mine) & (earlier < c * 32 + seq_col)
        columns.append(mine * 16 + jnp.sum(same.astype(jnp.int32), axis=1, keepdims=True))
    weights = [column(weight_ref[c : c + 1, :]) for c in range(4)]
    for k in range(4):
        for j in range(8):
            at = iota((32, 128), 1) + (j * 128 - k * 4)
            share = jnp.zeros((32, 128), F32)
            for c in range(4):
                share = jnp.where(at == columns[c], weights[c], share)
            upper = share.astype(BF16)
            take[k * 32 : (k + 1) * 32, j * 128 : (j + 1) * 128] = upper
            take[128 + k * 32 : 160 + k * 32, j * 128 : (j + 1) * 128] = (
                share - upper.astype(F32)
            ).astype(BF16)

    upper_row = iota((8, 64), 0)

    def renew(s, carry):
        for h in range(4):
            minus, given, strong_row, blended_row, decay_row = [
                rows_scr[n, h, pl.ds(s, 1), :] for n in range(5)
            ]
            zero = jnp.zeros((8, 64), F32)
            left = jnp.where(upper_row == 0, minus, jnp.where(upper_row == 1, given, zero))
            right = jnp.where(upper_row == 0, strong_row, jnp.where(upper_row == 1, blended_row, zero))
            change = lax.dot_general(
                left, right, (((0,), (0,)), ((), ())),
                preferred_element_type=F32, precision=lax.Precision.HIGHEST,
            )
            state[s, h] = old_state[s, h] * decay_row + change
        return carry

    lax.fori_loop(0, EARLY, renew, 0)

    def wait_bytes(ref, sem):
        pltpu.make_async_copy(ref, ref, sem).wait()

    g_copies = []
    for n, group in enumerate(ORDER):
        first = group * NS
        count = NS - 1 if group == 0 else NS
        wait_bytes(recv_a.at[pl.ds(first, count)], a_rsem.at[group])
        tiles = recv_a[first : first + NS].reshape(NS * 16, 128)
        gathered[n, tp] = dot(pick[...], tiles).astype(BF16)
        for d in (2, 1, 3):
            copy = pltpu.make_async_remote_copy(
                src_ref=gathered.at[n, tp], dst_ref=gathered.at[n, tp],
                send_sem=g_ssem.at[n, d - 1], recv_sem=g_rsem.at[n, d - 1],
                device_id={"tp": lax.rem(tp + d, N_TP)}, device_id_type=MESH,
            )
            copy.start()
            g_copies.append(copy)
    for load in loads:
        load.wait()
    d_copies = []
    for n, group in enumerate(ORDER):
        for copy in g_copies[3 * n : 3 * n + 3]:
            copy.wait_recv()
        rows, sums = [], None
        for t in range(N_TP):
            for k in range(4):
                rows.append(gathered[n, t, k * 3 * NS : (k + 1) * 3 * NS, :])
            part = gathered[n, t, KEPT:PACKED, :].astype(F32)
            sums = part if sums is None else sums + part
        rows = jnp.concatenate(rows, axis=1)
        square = jnp.concatenate(
            [sums[:, j : j + 1] + sums[:, 3 + j : 4 + j] for j in range(SLOTS)], axis=0
        )
        scale = lax.rsqrt(square * (1.0 / 2048.0) + NORM_EPS)
        gate = jnp.minimum(dot(rows, wg[...]) * scale, GATE_LIMIT)
        up = jnp.clip(dot(rows, wu[...]) * scale, -GATE_LIMIT, GATE_LIMIT)
        act = ((up + 1.0) * gate * jax.nn.sigmoid(GATE_SLOPE * gate)).astype(BF16)
        for j in range(N_TP):
            terms = dot(act, wd[:, j * 512 : (j + 1) * 512]).astype(BF16)
            for k in range(4):
                down_send[n, j, k * 3 * NS : (k + 1) * 3 * NS, :] = terms[
                    :, k * 128 : (k + 1) * 128
                ]
        for d in (2, 1, 3):
            peer = lax.rem(tp + d, N_TP)
            copy = pltpu.make_async_remote_copy(
                src_ref=down_send.at[n, peer], dst_ref=down_recv.at[n, d - 1],
                send_sem=d_ssem.at[n, d - 1], recv_sem=d_rsem.at[n, d - 1],
                device_id={"tp": peer}, device_id_type=MESH,
            )
            copy.start()
            d_copies.append(copy)

    def back_copy(r):
        return pltpu.make_async_remote_copy(
            src_ref=send_b.at[r], dst_ref=recv_b.at[me],
            send_sem=b_ssem, recv_sem=b_rsem,
            device_id={"ep": lax.rem(me + r, N_EP)}, device_id_type=MESH,
        )

    for n, group in enumerate(ORDER):
        for copy in d_copies[3 * n : 3 * n + 3]:
            copy.wait_recv()
        total = down_send[n, tp].astype(F32)
        for d in range(N_TP - 1):
            total = total + down_recv[n, d].astype(F32)
        first = group * NS
        send_b[first : first + NS] = (
            dot(unpick[...], total.astype(BF16)).astype(BF16).reshape(NS, 16, 128)
        )

        def send_back(r, carry):
            back_copy(r).start()
            return carry

        lax.fori_loop(max(1, first), first + NS, send_back, 0)
    recv_b[me] = send_b[0]
    lax.fori_loop(EARLY, 32, renew, 0)
    some = pl.ds(0, N_EP - 1)
    wait_bytes(recv_b.at[some], b_rsem)
    result = dot(take[...], recv_b[...].reshape(N_EP * 16, 128))
    for k in range(4):
        part = result[k * 32 : (k + 1) * 32] + result[128 + k * 32 : 160 + k * 32]
        out_ref[:, k * 128 : (k + 1) * 128] = (
            residual[:, k * 128 : (k + 1) * 128] + part
        ).astype(BF16)
    for copy in g_copies + d_copies:
        copy.wait_send()
    wait_bytes(send_a.at[some], a_ssem)
    wait_bytes(send_b.at[some], b_ssem)


def layer(gathered, wg, wu, wd):
    vmem = pl.BlockSpec(memory_space=pltpu.VMEM)
    hbm = pl.BlockSpec(memory_space=pltpu.HBM)
    dma = pltpu.SemaphoreType.DMA
    return pl.pallas_call(
        layer_kernel,
        out_shape=(
            pltpu.VMEM((32, 512), BF16),
            pltpu.VMEM((32, 4, 64, 64), F32),
        ),
        in_specs=[vmem] * 20 + [hbm] * 3,
        out_specs=(vmem, vmem),
        scratch_shapes=[
            pltpu.VMEM((1, 256), F32),
            pltpu.VMEM((1, 128), jnp.int32),
            pltpu.VMEM((4, 256), jnp.int32),
            pltpu.VMEM((32, 256), F32),
            pltpu.VMEM((32, 256), F32),
            pltpu.VMEM((5, 4, 32, 64), F32),
            pltpu.VMEM((2048, 256), BF16),
            pltpu.VMEM((2048, 256), BF16),
            pltpu.VMEM((256, 2048), BF16),
            pltpu.VMEM((1024, 256), BF16),
            pltpu.VMEM((256, 1024), BF16),
            pltpu.VMEM((PACKED, 16 * NS), BF16),
            pltpu.VMEM((16 * NS, KEPT), BF16),
            pltpu.VMEM((N_TP, 32, 512), BF16),
            pltpu.VMEM((N_TP - 1, 32, 512), BF16),
            pltpu.VMEM((32, 512), F32),
            pltpu.VMEM((N_EP, 16, 128), BF16),
            pltpu.VMEM((N_EP, 16, 128), BF16),
            pltpu.VMEM((GROUPS, N_TP, PACKED, 128), BF16),
            pltpu.VMEM((GROUPS, N_TP, KEPT, 128), BF16),
            pltpu.VMEM((GROUPS, N_TP - 1, KEPT, 128), BF16),
            pltpu.VMEM((N_EP, 16, 128), BF16),
            pltpu.VMEM((N_EP, 16, 128), BF16),
            dma((3,)),
            dma((N_TP - 1,)),
            dma((N_TP - 1,)),
            dma,
            dma((GROUPS,)),
            dma((GROUPS, N_TP - 1)),
            dma((GROUPS, N_TP - 1)),
            dma((GROUPS, N_TP - 1)),
            dma((GROUPS, N_TP - 1)),
            dma,
            dma,
        ],
        name="layer",
        compiler_params=pltpu.CompilerParams(
            collective_id=1, has_side_effects=True, vmem_limit_bytes=24 * 1024 * 1024
        ),
    )(*gathered, pin(wg), pin(wu), pin(wd))


def shards(
    tokens,
    previous,
    first_norm_gain,
    token_shift_share,
    receptance_weight,
    key_weight,
    value_weight,
    decay_down_map,
    decay_up_map,
    decay_offset,
    strength_down_map,
    strength_up_map,
    removal_key_scale,
    key_damping,
    self_term_weight,
    head_norm_gain,
    output_weight,
    state,
    second_norm_gain,
    routes,
    chosen_expert_weight,
    expert_gate_weight,
    expert_up_weight,
    expert_down_weight,
):
    gathered = gather(
        tokens, previous,
        [
            first_norm_gain.reshape(1, 2048), token_shift_share, decay_offset.reshape(1, 256),
            removal_key_scale.reshape(1, 256), key_damping.reshape(1, 256), self_term_weight,
            head_norm_gain.reshape(1, 256), second_norm_gain.reshape(1, 2048), routes.T,
            chosen_expert_weight.T, decay_down_map, strength_down_map, key_weight,
            receptance_weight, value_weight, decay_up_map, strength_up_map, state, output_weight,
        ],
    )
    return layer(gathered, expert_gate_weight, expert_up_weight, expert_down_weight)


def solution(mesh):
    in_specs = (
        P("ep", "tp"),
        P("ep", "tp"),
        P(),
        P(),
        P(None, "tp"),
        P(None, "tp"),
        P(None, "tp"),
        P(),
        P(),
        P("tp"),
        P(),
        P(),
        P("tp"),
        P("tp"),
        P("tp", None),
        P("tp"),
        P("tp", None),
        P("ep", "tp", None, None),
        P(),
        P("ep", None),
        P("ep", None),
        P("ep", None, "tp"),
        P("ep", None, "tp"),
        P("ep", "tp", None),
    )
    out_specs = (P("ep", "tp"), P("ep", "tp", None, None))
    return jax.shard_map(shards, mesh=mesh, in_specs=in_specs, out_specs=out_specs, check_vma=False)
```

```python
import jax
import jax.numpy as jnp
from jax import lax
from jax.experimental import pallas as pl
from jax.experimental.pallas import tpu as pltpu
from jax.sharding import PartitionSpec as P

NORM_EPS = 1e-06
GROUP_EPS = 0.00064
KEY_EPS = 1e-06
GATE_LIMIT = 7.0
GATE_SLOPE = 1.702


MESH = pl.DeviceIdType.MESH
N_EP = 64
N_TP = 4
GROUPS = 4
NS = N_EP // GROUPS
ORDER = (0, 3, 1, 2)
RELAYED = (0, 1, 1, 1)
EARLY = 15
SLOTS = 3
KEPT = 4 * SLOTS * NS
PACKED = KEPT + NS
CUT = 104
F32 = jnp.float32
BF16 = jnp.bfloat16


def pin(value):
    return pltpu.with_memory_space_constraint(value, pltpu.HBM)


def dot(a, b):
    return jnp.dot(a, b, preferred_element_type=F32)


def iota(shape, dim):
    return lax.broadcasted_iota(jnp.int32, shape, dim)


def third(m):
    return (m * 11) >> 5


def kept_row(m):
    return jnp.where(m == 12, 3, m + third(m))


def gather_kernel(
    tokens_hbm, previous_hbm, *refs,
):
    kept = len(PARTS)
    sources, (rows_ref, *targets) = refs[:kept], refs[kept : 2 * kept + 1]
    load_sem, part_sem, send_sem, recv_sem = refs[2 * kept + 1 :]
    tp = lax.axis_index("tp")
    loads = [
        pltpu.make_async_copy(tokens_hbm, rows_ref.at[tp, pl.ds(0, 32)], load_sem.at[0]),
        pltpu.make_async_copy(previous_hbm, rows_ref.at[tp, pl.ds(32, 32)], load_sem.at[1]),
    ]
    for load in loads:
        load.start()
    barrier = pltpu.get_barrier_semaphore()
    for d in range(1, N_TP):
        pl.semaphore_signal(
            barrier, inc=1, device_id={"tp": lax.rem(tp + d, N_TP)}, device_id_type=MESH
        )
    part_loads = []
    for n, (source, target, (shape, dtype, cut)) in enumerate(zip(sources, targets, PARTS)):
        if cut:
            source = source.at[:, pl.ds(pl.multiple_of(tp * cut, cut), cut)]
        load = pltpu.make_async_copy(source, target, part_sem.at[n])
        load.start()
        part_loads.append(load)
    for load in loads:
        load.wait()
    pl.semaphore_wait(barrier, N_TP - 1)
    copies = []
    for d in (2, 1, 3):
        copy = pltpu.make_async_remote_copy(
            src_ref=rows_ref.at[tp], dst_ref=rows_ref.at[tp],
            send_sem=send_sem.at[d - 1], recv_sem=recv_sem.at[d - 1],
            device_id={"tp": lax.rem(tp + d, N_TP)}, device_id_type=MESH,
        )
        copy.start()
        copies.append(copy)
    for load in part_loads:
        load.wait()
    for copy in copies:
        copy.wait()


PARTS = [
    ((1, 2048), F32, 0),
    ((5, 2048), F32, 0),
    ((1, 256), F32, 0),
    ((1, 256), F32, 0),
    ((1, 256), F32, 0),
    ((4, 64), F32, 0),
    ((1, 256), F32, 0),
    ((1, 512), F32, 512),
    ((4, 32), jnp.int32, 0),
    ((4, 32), F32, 0),
    ((2048, 128), BF16, 0),
    ((2048, 128), BF16, 0),
    ((2048, 256), BF16, 0),
    ((2048, 256), BF16, 0),
    ((2048, 256), BF16, 0),
    ((128, 256), BF16, 256),
    ((128, 256), BF16, 256),
    ((32, 4, 64, 64), F32, 0),
    ((256, 2048), BF16, 0),
]


def gather(tokens, previous, parts):
    hbm = pl.BlockSpec(memory_space=pltpu.HBM)
    vmem = pl.BlockSpec(memory_space=pltpu.VMEM)
    dma = pltpu.SemaphoreType.DMA
    return pl.pallas_call(
        gather_kernel,
        out_shape=[pltpu.VMEM((N_TP, 64, 512), BF16)]
        + [pltpu.VMEM(shape, dtype) for shape, dtype, _ in PARTS],
        in_specs=[hbm] * (2 + len(PARTS)),
        out_specs=[vmem] * (1 + len(PARTS)),
        scratch_shapes=[dma((2,)), dma((len(PARTS),)), dma((N_TP - 1,)), dma((N_TP - 1,))],
        name="gather",
        compiler_params=pltpu.CompilerParams(
            collective_id=0, has_side_effects=True, vmem_limit_bytes=16 * 1024 * 1024
        ),
    )(pin(tokens), pin(previous), *map(pin, parts))


def head_sums(values):
    same = iota((256, 256), 0) // 64 == iota((256, 256), 1) // 64
    return jnp.dot(
        values, same.astype(F32), preferred_element_type=F32, precision=lax.Precision.HIGHEST
    )


def column(row):
    eye = iota((32, 32), 0) == iota((32, 32), 1)
    return jnp.sum(jnp.where(eye, row, jnp.zeros_like(row)), axis=1, keepdims=True)


def layer_kernel(
    rows_ref,
    gain_one_ref, share_ref, offset_ref, key_scale_ref, damping_ref, self_pair, head_gain_ref,
    gain_ref, routes_ref, weight_ref, dd, sd, wk, wr, wv, du, su, old_state, wout,
    wg_hbm, wu_hbm, wd_hbm,
    out_ref, state,
    self_ref, routes_row_ref, routes_tiled_ref, along_scr, query_scr, rows_scr,
    wg, wu, wd, place, take, pick, unpick,
    rs_send, rs_recv, residual, send_a, recv_a, gathered, down_send, down_recv, send_b, recv_b,
    w_sem, rs_ssem, rs_rsem, a_ssem, a_rsem, g_ssem, g_rsem, d_ssem, d_rsem, b_ssem, b_rsem,
):
    me = lax.axis_index("ep")
    tp = lax.axis_index("tp")
    loads = [
        pltpu.make_async_copy(wg_hbm.at[0], wg, w_sem.at[0]),
        pltpu.make_async_copy(wu_hbm.at[0], wu, w_sem.at[1]),
        pltpu.make_async_copy(wd_hbm.at[0], wd, w_sem.at[2]),
    ]
    for load in loads:
        load.start()
    barrier = pltpu.get_barrier_semaphore()
    for d in range(1, N_TP):
        pl.semaphore_signal(
            barrier, inc=1, device_id={"tp": lax.rem(tp + d, N_TP)}, device_id_type=MESH
        )

    def greet(d, carry):
        pl.semaphore_signal(
            barrier, inc=1, device_id={"ep": lax.rem(me + d, N_EP)}, device_id_type=MESH
        )
        return carry

    lax.fori_loop(1, N_EP, greet, 0)

    for h in range(4):
        self_ref[:, h * 64 : (h + 1) * 64] = self_pair[h : h + 1, :]
    for c in range(4):
        routes_row_ref[:, c * 32 : (c + 1) * 32] = routes_ref[c : c + 1, :]
    for b in range(8):
        routes_tiled_ref[:, b * 32 : (b + 1) * 32] = routes_ref[...]
    square = jnp.zeros((32, 1), F32)
    for t in range(N_TP):
        part = rows_ref[t, 0:32, :].astype(F32)
        square = square + jnp.sum(part * part, axis=1, keepdims=True)
    scale = lax.rsqrt(square * (1.0 / 2048.0) + NORM_EPS)
    sums = [None] * 5
    for t in range(N_TP):
        span = slice(t * 512, (t + 1) * 512)
        normed = rows_ref[t, 0:32, :].astype(F32) * scale * gain_one_ref[:, span]
        change = rows_ref[t, 32:64, :].astype(F32) - normed
        for n, (m, weight) in enumerate([(3, dd), (4, sd), (1, wk), (0, wr), (2, wv)]):
            shifted = (normed + change * share_ref[m : m + 1, span]).astype(BF16)
            term = dot(shifted, weight[span, :])
            sums[n] = term if t == 0 else sums[n] + term
    low, strength_low, key, receptance, value = sums
    decay = dot(jnp.tanh(low).astype(BF16), du[...]) + offset_ref[...]
    decay = jnp.exp(jax.nn.sigmoid(decay) * -(2.718281828459045 ** -0.5))
    alpha = jax.nn.sigmoid(dot(strength_low.astype(BF16), su[...]))
    removal = key * key_scale_ref[...]
    removal = removal * lax.rsqrt(head_sums(removal * removal) + KEY_EPS)
    blended = key * (1.0 + (alpha - 1.0) * damping_ref[...])
    strong = removal * alpha
    query = decay * receptance
    both = head_sums(
        jnp.concatenate(
            [strong * receptance, blended * receptance, blended * receptance * self_ref[...]], axis=0
        )
    )
    for h in range(4):
        lanes = slice(h * 64, (h + 1) * 64)
        asked = jnp.concatenate([removal[:, lanes], query[:, lanes]], axis=0).astype(BF16)
        for q in range(8):
            held = old_state[4 * q : 4 * q + 4, h].reshape(256, 64).astype(BF16)
            answer = lax.dot_general(
                asked, held, (((1,), (1,)), ((), ())), preferred_element_type=F32
            )
            for j in range(4):
                s = 4 * q + j
                span = slice(j * 64, (j + 1) * 64)
                along_scr[s : s + 1, lanes] = answer[s : s + 1, span]
                query_scr[s : s + 1, lanes] = answer[32 + s : 33 + s, span]
    along = along_scr[...]
    readout = query_scr[...] - along * both[0:32] + value * both[32:64]
    centred = readout - head_sums(readout) * (1.0 / 64.0)
    spread = head_sums(centred * centred) * (1.0 / 64.0)
    mixed = centred * lax.rsqrt(spread + GROUP_EPS) * head_gain_ref[...] + both[64:96] * value
    mixed = mixed.astype(BF16)
    for n, values in enumerate((-along, value, strong, blended, decay)):
        for h in range(4):
            rows_scr[n, h] = values[:, h * 64 : (h + 1) * 64]

    for j in range(N_TP):
        rs_send[j] = dot(mixed, wout[:, j * 512 : (j + 1) * 512]).astype(BF16)
    pl.semaphore_wait(barrier, N_EP - 1 + N_TP - 1)
    rs_copies = []
    for d in (2, 1, 3):
        peer = lax.rem(tp + d, N_TP)
        copy = pltpu.make_async_remote_copy(
            src_ref=rs_send.at[peer], dst_ref=rs_recv.at[d - 1],
            send_sem=rs_ssem.at[d - 1], recv_sem=rs_rsem.at[d - 1],
            device_id={"tp": peer}, device_id_type=MESH,
        )
        copy.start()
        rs_copies.append(copy)

    lane = iota((1, 256), 1)
    block, seq = lane // 32, lane % 32
    source = iota((32, 256), 0)
    routed = [column(routes_ref[c : c + 1, :]) for c in range(4)]
    targets = []
    for c in range(4):
        mine = routes_tiled_ref[c : c + 1, :]
        rank = jnp.zeros((1, 256), jnp.int32)
        for other in range(c + 1):
            same = routed[other] == mine
            if other == c:
                same = same & (source < seq)
            rank = rank + jnp.sum(same.astype(jnp.int32), axis=0, keepdims=True)
        row = jnp.where(block < 4, block * 4 + rank, jnp.where(rank == block - 4, 3, -4096))
        targets.append(mine * 16 + row)

    def fill_place(i, carry):
        at = pl.multiple_of(i * 128, 128)
        row = iota((128, 256), 0) + at
        hit = row == targets[0]
        for c in range(1, 4):
            hit = hit | (row == targets[c])
        place[pl.ds(at, 128), :] = hit.astype(F32).astype(BF16)
        return carry

    lax.fori_loop(0, 8, fill_place, 0)

    piece, tile_row = iota((PACKED, 16 * NS), 0), iota((PACKED, 16 * NS), 1)
    pick[...] = (tile_row == (piece % NS) * 16 + kept_row(piece // NS)).astype(F32).astype(BF16)
    tile_row, piece = iota((16 * NS, KEPT), 0), iota((16 * NS, KEPT), 1)
    unpick[...] = (tile_row == (piece % NS) * 16 + kept_row(piece // NS)).astype(F32).astype(BF16)

    for copy in rs_copies:
        copy.wait()
    total = rows_ref[tp, 0:32, :].astype(F32) + rs_send[tp].astype(F32)
    for d in range(N_TP - 1):
        total = total + rs_recv[d].astype(F32)
    residual[...] = total
    square = jnp.sum(total * total, axis=1, keepdims=True)
    high = square.astype(BF16).astype(F32)
    low = square - high
    scaled = total * gain_ref[...]
    stack = [scaled[:, k * 128 : (k + 1) * 128] for k in range(4)]
    sum_lane = iota((32, 128), 1)
    for j in range(SLOTS):
        stack.append(jnp.where(sum_lane == j, high, jnp.where(sum_lane == 3 + j, low, 0.0)))
    stack.append(jnp.zeros((32, 128), F32))
    stack = jnp.concatenate(stack, axis=0).astype(BF16)
    send_a[...] = dot(place[...], stack).astype(BF16).reshape(N_EP, 16, 128)

    def out_copy(r, group):
        peer = lax.rem(me + N_EP - r, N_EP)
        return pltpu.make_async_remote_copy(
            src_ref=send_a.at[peer], dst_ref=recv_a.at[r],
            send_sem=a_ssem, recv_sem=a_rsem.at[group],
            device_id={"ep": peer}, device_id_type=MESH,
        )

    for group in ORDER:

        def send_out(r, carry, group=group):
            out_copy(r, group).start()
            return carry

        lax.fori_loop(max(1, group * NS), (group + 1) * NS, send_out, 0)
    recv_a[0] = send_a[me]

    seq_col = iota((32, 128), 0)
    earlier = iota((32, 128), 1)
    columns = []
    for c in range(4):
        mine = routed[c]
        same = (routes_row_ref[...] == mine) & (earlier < c * 32 + seq_col)
        columns.append(mine * 16 + jnp.sum(same.astype(jnp.int32), axis=1, keepdims=True))
    weights = [column(weight_ref[c : c + 1, :]) for c in range(4)]
    for k in range(4):
        for j in range(8):
            at = iota((32, 128), 1) + (j * 128 - k * 4)
            share = jnp.zeros((32, 128), F32)
            for c in range(4):
                share = jnp.where(at == columns[c], weights[c], share)
            upper = share.astype(BF16)
            take[k * 32 : (k + 1) * 32, j * 128 : (j + 1) * 128] = upper
            take[128 + k * 32 : 160 + k * 32, j * 128 : (j + 1) * 128] = (
                share - upper.astype(F32)
            ).astype(BF16)

    upper_row = iota((8, 64), 0)

    def renew(s, carry):
        for h in range(4):
            minus, given, strong_row, blended_row, decay_row = [
                rows_scr[n, h, pl.ds(s, 1), :] for n in range(5)
            ]
            zero = jnp.zeros((8, 64), F32)
            left = jnp.where(upper_row == 0, minus, jnp.where(upper_row == 1, given, zero))
            right = jnp.where(upper_row == 0, strong_row, jnp.where(upper_row == 1, blended_row, zero))
            change = lax.dot_general(
                left, right, (((0,), (0,)), ((), ())),
                preferred_element_type=F32, precision=lax.Precision.HIGHEST,
            )
            state[s, h] = old_state[s, h] * decay_row + change
        return carry

    lax.fori_loop(0, EARLY, renew, 0)

    def wait_bytes(ref, sem):
        pltpu.make_async_copy(ref, ref, sem).wait()

    ahead, behind = lax.rem(tp + 1, N_TP), lax.rem(tp + 3, N_TP)
    across = lax.rem(tp + 2, N_TP)
    sent = []

    def send(peer, source, target, send_sem, recv_sem):
        copy = pltpu.make_async_remote_copy(
            src_ref=source, dst_ref=target, send_sem=send_sem, recv_sem=recv_sem,
            device_id={"tp": peer}, device_id_type=MESH,
        )
        copy.start()
        sent.append(copy)
        return copy

    own_up, own_down, far_up, far_down = {}, {}, {}, {}

    def collect(n):
        first = ORDER[n] * NS
        count = NS - 1 if ORDER[n] == 0 else NS
        wait_bytes(recv_a.at[pl.ds(first, count)], a_rsem.at[ORDER[n]])
        tiles = recv_a[first : first + NS].reshape(NS * 16, 128)
        gathered[n, tp] = dot(pick[...], tiles).astype(BF16)
        mine = gathered.at[n, tp]
        own_up[n] = send(ahead, mine, mine, g_ssem.at[n, 0], g_rsem.at[n, 0])
        own_down[n] = send(behind, mine, mine, g_ssem.at[n, 1], g_rsem.at[n, 1])
        if not RELAYED[n]:
            far_up[n] = send(across, mine, mine, g_ssem.at[n, 2], g_rsem.at[n, 2])

    def pass_on(n):
        own_up[n].wait_recv()
        part = gathered.at[n, behind, pl.ds(0, CUT)]
        far_up[n] = send(ahead, part, part, g_ssem.at[n, 2], g_rsem.at[n, 2])
        own_down[n].wait_recv()
        part = gathered.at[n, ahead, pl.ds(CUT, PACKED - CUT)]
        far_down[n] = send(behind, part, part, g_ssem.at[n, 3], g_rsem.at[n, 3])

    arriving = {}

    def experts(n):
        far_up[n].wait_recv()
        if RELAYED[n]:
            far_down[n].wait_recv()
        else:
            own_up[n].wait_recv()
            own_down[n].wait_recv()
        rows, sums = [], None
        for t in range(N_TP):
            for k in range(4):
                rows.append(gathered[n, t, k * 3 * NS : (k + 1) * 3 * NS, :])
            part = gathered[n, t, KEPT:PACKED, :].astype(F32)
            sums = part if sums is None else sums + part
        rows = jnp.concatenate(rows, axis=1)
        square = jnp.concatenate(
            [sums[:, j : j + 1] + sums[:, 3 + j : 4 + j] for j in range(SLOTS)], axis=0
        )
        scale = lax.rsqrt(square * (1.0 / 2048.0) + NORM_EPS)
        gate = jnp.minimum(dot(rows, wg[...]) * scale, GATE_LIMIT)
        up = jnp.clip(dot(rows, wu[...]) * scale, -GATE_LIMIT, GATE_LIMIT)
        act = ((up + 1.0) * gate * jax.nn.sigmoid(GATE_SLOPE * gate)).astype(BF16)
        for j in range(N_TP):
            terms = dot(act, wd[:, j * 512 : (j + 1) * 512]).astype(BF16)
            for k in range(4):
                down_send[n, j, k * 3 * NS : (k + 1) * 3 * NS, :] = terms[
                    :, k * 128 : (k + 1) * 128
                ]
        for peer, slot in ((across, 2), (ahead, 0), (behind, 1)):
            copy = send(
                peer, down_send.at[n, peer], down_recv.at[n, slot],
                d_ssem.at[n, slot], d_rsem.at[n, slot],
            )
            arriving.setdefault(n, []).append(copy)

    def back_copy(r):
        return pltpu.make_async_remote_copy(
            src_ref=send_b.at[r], dst_ref=recv_b.at[me],
            send_sem=b_ssem, recv_sem=b_rsem,
            device_id={"ep": lax.rem(me + r, N_EP)}, device_id_type=MESH,
        )

    def send_back(r, carry):
        back_copy(r).start()
        return carry

    def give_back(n):
        for copy in arriving[n]:
            copy.wait_recv()
        total = down_send[n, tp].astype(F32)
        for d in range(len(arriving[n])):
            total = total + down_recv[n, d].astype(F32)
        first = ORDER[n] * NS
        send_b[first : first + NS] = (
            dot(unpick[...], total.astype(BF16)).astype(BF16).reshape(NS, 16, 128)
        )
        lax.fori_loop(max(1, first), first + NS, send_back, 0)

    collect(0)
    collect(1)
    collect(2)
    collect(3)
    for load in loads:
        load.wait()
    experts(0)
    pass_on(1)
    pass_on(2)
    pass_on(3)
    experts(1)
    experts(2)
    experts(3)
    give_back(0)
    give_back(1)
    give_back(2)
    give_back(3)
    recv_b[me] = send_b[0]
    lax.fori_loop(EARLY, 32, renew, 0)
    some = pl.ds(0, N_EP - 1)
    wait_bytes(recv_b.at[some], b_rsem)
    result = dot(take[...], recv_b[...].reshape(N_EP * 16, 128))
    for k in range(4):
        part = result[k * 32 : (k + 1) * 32] + result[128 + k * 32 : 160 + k * 32]
        out_ref[:, k * 128 : (k + 1) * 128] = (
            residual[:, k * 128 : (k + 1) * 128] + part
        ).astype(BF16)
    for copy in sent:
        copy.wait_send()
    wait_bytes(send_a.at[some], a_ssem)
    wait_bytes(send_b.at[some], b_ssem)


def layer(gathered, wg, wu, wd):
    vmem = pl.BlockSpec(memory_space=pltpu.VMEM)
    hbm = pl.BlockSpec(memory_space=pltpu.HBM)
    dma = pltpu.SemaphoreType.DMA
    return pl.pallas_call(
        layer_kernel,
        out_shape=(
            pltpu.VMEM((32, 512), BF16),
            pltpu.VMEM((32, 4, 64, 64), F32),
        ),
        in_specs=[vmem] * 20 + [hbm] * 3,
        out_specs=(vmem, vmem),
        scratch_shapes=[
            pltpu.VMEM((1, 256), F32),
            pltpu.VMEM((1, 128), jnp.int32),
            pltpu.VMEM((4, 256), jnp.int32),
            pltpu.VMEM((32, 256), F32),
            pltpu.VMEM((32, 256), F32),
            pltpu.VMEM((5, 4, 32, 64), F32),
            pltpu.VMEM((2048, 256), BF16),
            pltpu.VMEM((2048, 256), BF16),
            pltpu.VMEM((256, 2048), BF16),
            pltpu.VMEM((1024, 256), BF16),
            pltpu.VMEM((256, 1024), BF16),
            pltpu.VMEM((PACKED, 16 * NS), BF16),
            pltpu.VMEM((16 * NS, KEPT), BF16),
            pltpu.VMEM((N_TP, 32, 512), BF16),
            pltpu.VMEM((N_TP - 1, 32, 512), BF16),
            pltpu.VMEM((32, 512), F32),
            pltpu.VMEM((N_EP, 16, 128), BF16),
            pltpu.VMEM((N_EP, 16, 128), BF16),
            pltpu.VMEM((GROUPS, N_TP, PACKED, 128), BF16),
            pltpu.VMEM((GROUPS, N_TP, KEPT, 128), BF16),
            pltpu.VMEM((GROUPS, 3, KEPT, 128), BF16),
            pltpu.VMEM((N_EP, 16, 128), BF16),
            pltpu.VMEM((N_EP, 16, 128), BF16),
            dma((3,)),
            dma((N_TP - 1,)),
            dma((N_TP - 1,)),
            dma,
            dma((GROUPS,)),
            dma((GROUPS, 4)),
            dma((GROUPS, 4)),
            dma((GROUPS, 4)),
            dma((GROUPS, 4)),
            dma,
            dma,
        ],
        name="layer",
        compiler_params=pltpu.CompilerParams(
            collective_id=1, has_side_effects=True, vmem_limit_bytes=24 * 1024 * 1024
        ),
    )(*gathered, pin(wg), pin(wu), pin(wd))


def store_kernel(out_ref, state_ref, out_hbm, state_hbm, sem):
    copies = [pltpu.make_async_copy(out_ref, out_hbm, sem.at[0])]
    for n in range(4):
        some = pl.ds(n * 8, 8)
        copies.append(
            pltpu.make_async_copy(state_ref.at[some], state_hbm.at[some], sem.at[1 + n])
        )
    for copy in copies:
        copy.start()
    for copy in copies:
        copy.wait()


def store(out, state):
    vmem = pl.BlockSpec(memory_space=pltpu.VMEM)
    hbm = pl.BlockSpec(memory_space=pl.ANY)
    return pl.pallas_call(
        store_kernel,
        out_shape=(
            jax.ShapeDtypeStruct(out.shape, out.dtype),
            jax.ShapeDtypeStruct(state.shape, state.dtype),
        ),
        in_specs=[vmem, vmem],
        out_specs=(hbm, hbm),
        scratch_shapes=[pltpu.SemaphoreType.DMA((5,))],
        name="store",
        compiler_params=pltpu.CompilerParams(vmem_limit_bytes=8 * 1024 * 1024),
    )(out, state)


def shards(
    tokens,
    previous,
    first_norm_gain,
    token_shift_share,
    receptance_weight,
    key_weight,
    value_weight,
    decay_down_map,
    decay_up_map,
    decay_offset,
    strength_down_map,
    strength_up_map,
    removal_key_scale,
    key_damping,
    self_term_weight,
    head_norm_gain,
    output_weight,
    state,
    second_norm_gain,
    routes,
    chosen_expert_weight,
    expert_gate_weight,
    expert_up_weight,
    expert_down_weight,
):
    gathered = gather(
        tokens, previous,
        [
            first_norm_gain.reshape(1, 2048), token_shift_share, decay_offset.reshape(1, 256),
            removal_key_scale.reshape(1, 256), key_damping.reshape(1, 256), self_term_weight,
            head_norm_gain.reshape(1, 256), second_norm_gain.reshape(1, 2048), routes.T,
            chosen_expert_weight.T, decay_down_map, strength_down_map, key_weight,
            receptance_weight, value_weight, decay_up_map, strength_up_map, state, output_weight,
        ],
    )
    return store(*layer(gathered, expert_gate_weight, expert_up_weight, expert_down_weight))


def solution(mesh):
    in_specs = (
        P("ep", "tp"),
        P("ep", "tp"),
        P(),
        P(),
        P(None, "tp"),
        P(None, "tp"),
        P(None, "tp"),
        P(),
        P(),
        P("tp"),
        P(),
        P(),
        P("tp"),
        P("tp"),
        P("tp", None),
        P("tp"),
        P("tp", None),
        P("ep", "tp", None, None),
        P(),
        P("ep", None),
        P("ep", None),
        P("ep", None, "tp"),
        P("ep", None, "tp"),
        P("ep", "tp", None),
    )
    out_specs = (P("ep", "tp"), P("ep", "tp", None, None))
    return jax.shard_map(shards, mesh=mesh, in_specs=in_specs, out_specs=out_specs, check_vma=False)
```

```python
import jax
import jax.numpy as jnp
from jax import lax
from jax.experimental import pallas as pl
from jax.experimental.pallas import tpu as pltpu
from jax.sharding import PartitionSpec as P

NORM_EPS = 1e-06
GROUP_EPS = 0.00064
KEY_EPS = 1e-06
GATE_LIMIT = 7.0
GATE_SLOPE = 1.702


MESH = pl.DeviceIdType.MESH
N_EP = 64
N_TP = 4
GROUPS = 4
NS = N_EP // GROUPS
ORDER = (0, 3, 1, 2)
RELAYED = (0, 1, 1, 1)
EARLY = 15
SLOTS = 3
KEPT = 4 * SLOTS * NS
PACKED = KEPT + NS
CUT = 104
F32 = jnp.float32
BF16 = jnp.bfloat16


def pin(value):
    return pltpu.with_memory_space_constraint(value, pltpu.HBM)


def dot(a, b):
    return jnp.dot(a, b, preferred_element_type=F32)


def iota(shape, dim):
    return lax.broadcasted_iota(jnp.int32, shape, dim)


def third(m):
    return (m * 11) >> 5


def kept_row(m):
    return jnp.where(m == 12, 3, m + third(m))


def gather_kernel(
    tokens_hbm, previous_hbm, *refs,
):
    kept = len(PARTS)
    sources, (rows_ref, *targets) = refs[:kept], refs[kept : 2 * kept + 1]
    load_sem, part_sem, send_sem, recv_sem = refs[2 * kept + 1 :]
    tp = lax.axis_index("tp")
    loads = [
        pltpu.make_async_copy(tokens_hbm, rows_ref.at[tp, pl.ds(0, 32)], load_sem.at[0]),
        pltpu.make_async_copy(previous_hbm, rows_ref.at[tp, pl.ds(32, 32)], load_sem.at[1]),
    ]
    for load in loads:
        load.start()
    barrier = pltpu.get_barrier_semaphore()
    for d in range(1, N_TP):
        pl.semaphore_signal(
            barrier, inc=1, device_id={"tp": lax.rem(tp + d, N_TP)}, device_id_type=MESH
        )
    part_loads = []
    for n, (source, target, (shape, dtype, cut)) in enumerate(zip(sources, targets, PARTS)):
        if cut:
            source = source.at[:, pl.ds(pl.multiple_of(tp * cut, cut), cut)]
        load = pltpu.make_async_copy(source, target, part_sem.at[n])
        load.start()
        part_loads.append(load)
    for load in loads:
        load.wait()
    pl.semaphore_wait(barrier, N_TP - 1)
    copies = []
    for d in (2, 1, 3):
        copy = pltpu.make_async_remote_copy(
            src_ref=rows_ref.at[tp], dst_ref=rows_ref.at[tp],
            send_sem=send_sem.at[d - 1], recv_sem=recv_sem.at[d - 1],
            device_id={"tp": lax.rem(tp + d, N_TP)}, device_id_type=MESH,
        )
        copy.start()
        copies.append(copy)
    for load in part_loads:
        load.wait()
    for copy in copies:
        copy.wait()


PARTS = [
    ((1, 2048), F32, 0),
    ((5, 2048), F32, 0),
    ((1, 256), F32, 0),
    ((1, 256), F32, 0),
    ((1, 256), F32, 0),
    ((4, 64), F32, 0),
    ((1, 256), F32, 0),
    ((1, 512), F32, 512),
    ((4, 32), jnp.int32, 0),
    ((4, 32), F32, 0),
    ((2048, 128), BF16, 0),
    ((2048, 128), BF16, 0),
    ((2048, 256), BF16, 0),
    ((2048, 256), BF16, 0),
    ((2048, 256), BF16, 0),
    ((128, 256), BF16, 256),
    ((128, 256), BF16, 256),
    ((32, 4, 64, 64), F32, 0),
    ((256, 2048), BF16, 0),
]


def gather(tokens, previous, parts):
    hbm = pl.BlockSpec(memory_space=pltpu.HBM)
    vmem = pl.BlockSpec(memory_space=pltpu.VMEM)
    dma = pltpu.SemaphoreType.DMA
    return pl.pallas_call(
        gather_kernel,
        out_shape=[pltpu.VMEM((N_TP, 64, 512), BF16)]
        + [pltpu.VMEM(shape, dtype) for shape, dtype, _ in PARTS],
        in_specs=[hbm] * (2 + len(PARTS)),
        out_specs=[vmem] * (1 + len(PARTS)),
        scratch_shapes=[dma((2,)), dma((len(PARTS),)), dma((N_TP - 1,)), dma((N_TP - 1,))],
        name="gather",
        compiler_params=pltpu.CompilerParams(
            collective_id=0, has_side_effects=True, vmem_limit_bytes=16 * 1024 * 1024
        ),
    )(pin(tokens), pin(previous), *map(pin, parts))


def head_sums(values):
    same = iota((256, 256), 0) // 64 == iota((256, 256), 1) // 64
    return jnp.dot(
        values, same.astype(F32), preferred_element_type=F32, precision=lax.Precision.HIGHEST
    )


def column(row):
    eye = iota((32, 32), 0) == iota((32, 32), 1)
    return jnp.sum(jnp.where(eye, row, jnp.zeros_like(row)), axis=1, keepdims=True)


def layer_kernel(
    rows_ref,
    gain_one_ref, share_ref, offset_ref, key_scale_ref, damping_ref, self_pair, head_gain_ref,
    gain_ref, routes_ref, weight_ref, dd, sd, wk, wr, wv, du, su, old_state, wout,
    wg_hbm, wu_hbm, wd_hbm,
    out_ref, state,
    self_ref, routes_row_ref, routes_tiled_ref, along_scr, query_scr, rows_scr,
    wg, wu, wd, place, take, pick, unpick,
    rs_send, rs_recv, residual, send_a, recv_a, gathered, down_send, down_recv, send_b, recv_b,
    w_sem, rs_ssem, rs_rsem, a_ssem, a_rsem, g_ssem, g_rsem, d_ssem, d_rsem, b_ssem, b_rsem,
):
    me = lax.axis_index("ep")
    tp = lax.axis_index("tp")
    loads = [
        pltpu.make_async_copy(wg_hbm.at[0], wg, w_sem.at[0]),
        pltpu.make_async_copy(wu_hbm.at[0], wu, w_sem.at[1]),
        pltpu.make_async_copy(wd_hbm.at[0], wd, w_sem.at[2]),
    ]
    for load in loads:
        load.start()
    barrier = pltpu.get_barrier_semaphore()
    for d in range(1, N_TP):
        pl.semaphore_signal(
            barrier, inc=1, device_id={"tp": lax.rem(tp + d, N_TP)}, device_id_type=MESH
        )

    def greet(d, carry):
        pl.semaphore_signal(
            barrier, inc=1, device_id={"ep": lax.rem(me + d, N_EP)}, device_id_type=MESH
        )
        return carry

    lax.fori_loop(20, 44, greet, 0, unroll=4)
    lax.fori_loop(4, 20, greet, 0, unroll=4)
    lax.fori_loop(44, N_EP, greet, 0, unroll=4)
    lax.fori_loop(1, 4, greet, 0)

    for h in range(4):
        self_ref[:, h * 64 : (h + 1) * 64] = self_pair[h : h + 1, :]
    for c in range(4):
        routes_row_ref[:, c * 32 : (c + 1) * 32] = routes_ref[c : c + 1, :]
    for b in range(8):
        routes_tiled_ref[:, b * 32 : (b + 1) * 32] = routes_ref[...]
    square = jnp.zeros((32, 1), F32)
    for t in range(N_TP):
        part = rows_ref[t, 0:32, :].astype(F32)
        square = square + jnp.sum(part * part, axis=1, keepdims=True)
    scale = lax.rsqrt(square * (1.0 / 2048.0) + NORM_EPS)
    sums = [None] * 5
    for t in range(N_TP):
        span = slice(t * 512, (t + 1) * 512)
        normed = rows_ref[t, 0:32, :].astype(F32) * scale * gain_one_ref[:, span]
        change = rows_ref[t, 32:64, :].astype(F32) - normed
        for n, (m, weight) in enumerate([(3, dd), (4, sd), (1, wk), (0, wr), (2, wv)]):
            shifted = (normed + change * share_ref[m : m + 1, span]).astype(BF16)
            term = dot(shifted, weight[span, :])
            sums[n] = term if t == 0 else sums[n] + term
    low, strength_low, key, receptance, value = sums
    decay = dot(jnp.tanh(low).astype(BF16), du[...]) + offset_ref[...]
    decay = jnp.exp(jax.nn.sigmoid(decay) * -(2.718281828459045 ** -0.5))
    alpha = jax.nn.sigmoid(dot(strength_low.astype(BF16), su[...]))
    removal = key * key_scale_ref[...]
    removal = removal * lax.rsqrt(head_sums(removal * removal) + KEY_EPS)
    blended = key * (1.0 + (alpha - 1.0) * damping_ref[...])
    strong = removal * alpha
    query = decay * receptance
    both = head_sums(
        jnp.concatenate(
            [strong * receptance, blended * receptance, blended * receptance * self_ref[...]], axis=0
        )
    )
    for h in range(4):
        lanes = slice(h * 64, (h + 1) * 64)
        asked = jnp.concatenate([removal[:, lanes], query[:, lanes]], axis=0).astype(BF16)
        for q in range(8):
            held = old_state[4 * q : 4 * q + 4, h].reshape(256, 64).astype(BF16)
            answer = lax.dot_general(
                asked, held, (((1,), (1,)), ((), ())), preferred_element_type=F32
            )
            for j in range(4):
                s = 4 * q + j
                span = slice(j * 64, (j + 1) * 64)
                along_scr[s : s + 1, lanes] = answer[s : s + 1, span]
                query_scr[s : s + 1, lanes] = answer[32 + s : 33 + s, span]
    along = along_scr[...]
    readout = query_scr[...] - along * both[0:32] + value * both[32:64]
    centred = readout - head_sums(readout) * (1.0 / 64.0)
    spread = head_sums(centred * centred) * (1.0 / 64.0)
    mixed = centred * lax.rsqrt(spread + GROUP_EPS) * head_gain_ref[...] + both[64:96] * value
    mixed = mixed.astype(BF16)
    for n, values in enumerate((-along, value, strong, blended, decay)):
        for h in range(4):
            rows_scr[n, h] = values[:, h * 64 : (h + 1) * 64]

    for j in range(N_TP):
        rs_send[j] = dot(mixed, wout[:, j * 512 : (j + 1) * 512]).astype(BF16)
    pl.semaphore_wait(barrier, N_EP - 1 + N_TP - 1)
    rs_copies = []
    for d in (2, 1, 3):
        peer = lax.rem(tp + d, N_TP)
        copy = pltpu.make_async_remote_copy(
            src_ref=rs_send.at[peer], dst_ref=rs_recv.at[d - 1],
            send_sem=rs_ssem.at[d - 1], recv_sem=rs_rsem.at[d - 1],
            device_id={"tp": peer}, device_id_type=MESH,
        )
        copy.start()
        rs_copies.append(copy)

    lane = iota((1, 256), 1)
    block, seq = lane // 32, lane % 32
    source = iota((32, 256), 0)
    routed = [column(routes_ref[c : c + 1, :]) for c in range(4)]
    targets = []
    for c in range(4):
        mine = routes_tiled_ref[c : c + 1, :]
        rank = jnp.zeros((1, 256), jnp.int32)
        for other in range(c + 1):
            same = routed[other] == mine
            if other == c:
                same = same & (source < seq)
            rank = rank + jnp.sum(same.astype(jnp.int32), axis=0, keepdims=True)
        row = jnp.where(block < 4, block * 4 + rank, jnp.where(rank == block - 4, 3, -4096))
        targets.append(mine * 16 + row)

    def fill_place(i, carry):
        at = pl.multiple_of(i * 128, 128)
        row = iota((128, 256), 0) + at
        hit = row == targets[0]
        for c in range(1, 4):
            hit = hit | (row == targets[c])
        place[pl.ds(at, 128), :] = hit.astype(F32).astype(BF16)
        return carry

    lax.fori_loop(0, 8, fill_place, 0)

    piece, tile_row = iota((PACKED, 16 * NS), 0), iota((PACKED, 16 * NS), 1)
    pick[...] = (tile_row == (piece % NS) * 16 + kept_row(piece // NS)).astype(F32).astype(BF16)
    tile_row, piece = iota((16 * NS, KEPT), 0), iota((16 * NS, KEPT), 1)
    unpick[...] = (tile_row == (piece % NS) * 16 + kept_row(piece // NS)).astype(F32).astype(BF16)

    for copy in rs_copies:
        copy.wait()
    total = rows_ref[tp, 0:32, :].astype(F32) + rs_send[tp].astype(F32)
    for d in range(N_TP - 1):
        total = total + rs_recv[d].astype(F32)
    residual[...] = total
    square = jnp.sum(total * total, axis=1, keepdims=True)
    high = square.astype(BF16).astype(F32)
    low = square - high
    scaled = total * gain_ref[...]
    stack = [scaled[:, k * 128 : (k + 1) * 128] for k in range(4)]
    sum_lane = iota((32, 128), 1)
    for j in range(SLOTS):
        stack.append(jnp.where(sum_lane == j, high, jnp.where(sum_lane == 3 + j, low, 0.0)))
    stack.append(jnp.zeros((32, 128), F32))
    stack = jnp.concatenate(stack, axis=0).astype(BF16)
    send_a[...] = dot(place[...], stack).astype(BF16).reshape(N_EP, 16, 128)

    def out_copy(r, group):
        peer = lax.rem(me + N_EP - r, N_EP)
        return pltpu.make_async_remote_copy(
            src_ref=send_a.at[peer], dst_ref=recv_a.at[r],
            send_sem=a_ssem, recv_sem=a_rsem.at[group],
            device_id={"ep": peer}, device_id_type=MESH,
        )

    for group in ORDER:

        def send_out(r, carry, group=group):
            out_copy(r, group).start()
            return carry

        lax.fori_loop(max(1, group * NS), (group + 1) * NS, send_out, 0, unroll=5 if group == 0 else 4)
    recv_a[0] = send_a[me]

    seq_col = iota((32, 128), 0)
    earlier = iota((32, 128), 1)
    columns = []
    for c in range(4):
        mine = routed[c]
        same = (routes_row_ref[...] == mine) & (earlier < c * 32 + seq_col)
        columns.append(mine * 16 + jnp.sum(same.astype(jnp.int32), axis=1, keepdims=True))
    weights = [column(weight_ref[c : c + 1, :]) for c in range(4)]
    for k in range(4):
        for j in range(8):
            at = iota((32, 128), 1) + (j * 128 - k * 4)
            share = jnp.zeros((32, 128), F32)
            for c in range(4):
                share = jnp.where(at == columns[c], weights[c], share)
            upper = share.astype(BF16)
            take[k * 32 : (k + 1) * 32, j * 128 : (j + 1) * 128] = upper
            take[128 + k * 32 : 160 + k * 32, j * 128 : (j + 1) * 128] = (
                share - upper.astype(F32)
            ).astype(BF16)

    upper_row = iota((8, 64), 0)

    def renew(s, carry):
        for h in range(4):
            minus, given, strong_row, blended_row, decay_row = [
                rows_scr[n, h, pl.ds(s, 1), :] for n in range(5)
            ]
            zero = jnp.zeros((8, 64), F32)
            left = jnp.where(upper_row == 0, minus, jnp.where(upper_row == 1, given, zero))
            right = jnp.where(upper_row == 0, strong_row, jnp.where(upper_row == 1, blended_row, zero))
            change = lax.dot_general(
                left, right, (((0,), (0,)), ((), ())),
                preferred_element_type=F32, precision=lax.Precision.HIGHEST,
            )
            state[s, h] = old_state[s, h] * decay_row + change
        return carry

    lax.fori_loop(0, EARLY, renew, 0)

    def wait_bytes(ref, sem):
        pltpu.make_async_copy(ref, ref, sem).wait()

    ahead, behind = lax.rem(tp + 1, N_TP), lax.rem(tp + 3, N_TP)
    across = lax.rem(tp + 2, N_TP)
    sent = []

    def send(peer, source, target, send_sem, recv_sem):
        copy = pltpu.make_async_remote_copy(
            src_ref=source, dst_ref=target, send_sem=send_sem, recv_sem=recv_sem,
            device_id={"tp": peer}, device_id_type=MESH,
        )
        copy.start()
        sent.append(copy)
        return copy

    own_up, own_down, far_up, far_down = {}, {}, {}, {}

    def collect(n):
        first = ORDER[n] * NS
        count = NS - 1 if ORDER[n] == 0 else NS
        wait_bytes(recv_a.at[pl.ds(first, count)], a_rsem.at[ORDER[n]])
        tiles = recv_a[first : first + NS].reshape(NS * 16, 128)
        gathered[n, tp] = dot(pick[...], tiles).astype(BF16)
        mine = gathered.at[n, tp]
        own_up[n] = send(ahead, mine, mine, g_ssem.at[n, 0], g_rsem.at[n, 0])
        own_down[n] = send(behind, mine, mine, g_ssem.at[n, 1], g_rsem.at[n, 1])
        if not RELAYED[n]:
            far_up[n] = send(across, mine, mine, g_ssem.at[n, 2], g_rsem.at[n, 2])

    def pass_on(n):
        own_up[n].wait_recv()
        part = gathered.at[n, behind, pl.ds(0, CUT)]
        far_up[n] = send(ahead, part, part, g_ssem.at[n, 2], g_rsem.at[n, 2])
        own_down[n].wait_recv()
        part = gathered.at[n, ahead, pl.ds(CUT, PACKED - CUT)]
        far_down[n] = send(behind, part, part, g_ssem.at[n, 3], g_rsem.at[n, 3])

    arriving = {}

    def experts(n):
        far_up[n].wait_recv()
        if RELAYED[n]:
            far_down[n].wait_recv()
        else:
            own_up[n].wait_recv()
            own_down[n].wait_recv()
        rows, sums = [], None
        for t in range(N_TP):
            for k in range(4):
                rows.append(gathered[n, t, k * 3 * NS : (k + 1) * 3 * NS, :])
            part = gathered[n, t, KEPT:PACKED, :].astype(F32)
            sums = part if sums is None else sums + part
        rows = jnp.concatenate(rows, axis=1)
        square = jnp.concatenate(
            [sums[:, j : j + 1] + sums[:, 3 + j : 4 + j] for j in range(SLOTS)], axis=0
        )
        scale = lax.rsqrt(square * (1.0 / 2048.0) + NORM_EPS)
        gate = jnp.minimum(dot(rows, wg[...]) * scale, GATE_LIMIT)
        up = jnp.clip(dot(rows, wu[...]) * scale, -GATE_LIMIT, GATE_LIMIT)
        act = ((up + 1.0) * gate * jax.nn.sigmoid(GATE_SLOPE * gate)).astype(BF16)
        for j in range(N_TP):
            terms = dot(act, wd[:, j * 512 : (j + 1) * 512]).astype(BF16)
            for k in range(4):
                down_send[n, j, k * 3 * NS : (k + 1) * 3 * NS, :] = terms[
                    :, k * 128 : (k + 1) * 128
                ]
        for peer, slot in ((across, 2), (ahead, 0), (behind, 1)):
            copy = send(
                peer, down_send.at[n, peer], down_recv.at[n, slot],
                d_ssem.at[n, slot], d_rsem.at[n, slot],
            )
            arriving.setdefault(n, []).append(copy)

    def back_copy(r):
        return pltpu.make_async_remote_copy(
            src_ref=send_b.at[r], dst_ref=recv_b.at[me],
            send_sem=b_ssem, recv_sem=b_rsem,
            device_id={"ep": lax.rem(me + r, N_EP)}, device_id_type=MESH,
        )

    def send_back(r, carry):
        back_copy(r).start()
        return carry

    def give_back(n):
        for copy in arriving[n]:
            copy.wait_recv()
        total = down_send[n, tp].astype(F32)
        for d in range(len(arriving[n])):
            total = total + down_recv[n, d].astype(F32)
        first = ORDER[n] * NS
        send_b[first : first + NS] = (
            dot(unpick[...], total.astype(BF16)).astype(BF16).reshape(NS, 16, 128)
        )
        lax.fori_loop(max(1, first), first + NS, send_back, 0, unroll=4 if first else 5)

    collect(0)
    collect(1)
    collect(2)
    collect(3)
    for load in loads:
        load.wait()
    experts(0)
    pass_on(1)
    pass_on(2)
    pass_on(3)
    experts(1)
    experts(2)
    experts(3)
    give_back(0)
    give_back(1)
    give_back(2)
    give_back(3)
    recv_b[me] = send_b[0]
    lax.fori_loop(EARLY, 32, renew, 0)
    some = pl.ds(0, N_EP - 1)
    wait_bytes(recv_b.at[some], b_rsem)
    result = dot(take[...], recv_b[...].reshape(N_EP * 16, 128))
    for k in range(4):
        part = result[k * 32 : (k + 1) * 32] + result[128 + k * 32 : 160 + k * 32]
        out_ref[:, k * 128 : (k + 1) * 128] = (
            residual[:, k * 128 : (k + 1) * 128] + part
        ).astype(BF16)
    for copy in sent:
        copy.wait_send()
    wait_bytes(send_a.at[some], a_ssem)
    wait_bytes(send_b.at[some], b_ssem)


def layer(gathered, wg, wu, wd):
    vmem = pl.BlockSpec(memory_space=pltpu.VMEM)
    hbm = pl.BlockSpec(memory_space=pltpu.HBM)
    dma = pltpu.SemaphoreType.DMA
    return pl.pallas_call(
        layer_kernel,
        out_shape=(
            pltpu.VMEM((32, 512), BF16),
            pltpu.VMEM((32, 4, 64, 64), F32),
        ),
        in_specs=[vmem] * 20 + [hbm] * 3,
        out_specs=(vmem, vmem),
        scratch_shapes=[
            pltpu.VMEM((1, 256), F32),
            pltpu.VMEM((1, 128), jnp.int32),
            pltpu.VMEM((4, 256), jnp.int32),
            pltpu.VMEM((32, 256), F32),
            pltpu.VMEM((32, 256), F32),
            pltpu.VMEM((5, 4, 32, 64), F32),
            pltpu.VMEM((2048, 256), BF16),
            pltpu.VMEM((2048, 256), BF16),
            pltpu.VMEM((256, 2048), BF16),
            pltpu.VMEM((1024, 256), BF16),
            pltpu.VMEM((256, 1024), BF16),
            pltpu.VMEM((PACKED, 16 * NS), BF16),
            pltpu.VMEM((16 * NS, KEPT), BF16),
            pltpu.VMEM((N_TP, 32, 512), BF16),
            pltpu.VMEM((N_TP - 1, 32, 512), BF16),
            pltpu.VMEM((32, 512), F32),
            pltpu.VMEM((N_EP, 16, 128), BF16),
            pltpu.VMEM((N_EP, 16, 128), BF16),
            pltpu.VMEM((GROUPS, N_TP, PACKED, 128), BF16),
            pltpu.VMEM((GROUPS, N_TP, KEPT, 128), BF16),
            pltpu.VMEM((GROUPS, 3, KEPT, 128), BF16),
            pltpu.VMEM((N_EP, 16, 128), BF16),
            pltpu.VMEM((N_EP, 16, 128), BF16),
            dma((3,)),
            dma((N_TP - 1,)),
            dma((N_TP - 1,)),
            dma,
            dma((GROUPS,)),
            dma((GROUPS, 4)),
            dma((GROUPS, 4)),
            dma((GROUPS, 4)),
            dma((GROUPS, 4)),
            dma,
            dma,
        ],
        name="layer",
        compiler_params=pltpu.CompilerParams(
            collective_id=1, has_side_effects=True, vmem_limit_bytes=24 * 1024 * 1024
        ),
    )(*gathered, pin(wg), pin(wu), pin(wd))


def store_kernel(out_ref, state_ref, out_hbm, state_hbm, sem):
    copies = [pltpu.make_async_copy(out_ref, out_hbm, sem.at[0])]
    for n in range(4):
        some = pl.ds(n * 8, 8)
        copies.append(
            pltpu.make_async_copy(state_ref.at[some], state_hbm.at[some], sem.at[1 + n])
        )
    for copy in copies:
        copy.start()
    for copy in copies:
        copy.wait()


def store(out, state):
    vmem = pl.BlockSpec(memory_space=pltpu.VMEM)
    hbm = pl.BlockSpec(memory_space=pl.ANY)
    return pl.pallas_call(
        store_kernel,
        out_shape=(
            jax.ShapeDtypeStruct(out.shape, out.dtype),
            jax.ShapeDtypeStruct(state.shape, state.dtype),
        ),
        in_specs=[vmem, vmem],
        out_specs=(hbm, hbm),
        scratch_shapes=[pltpu.SemaphoreType.DMA((5,))],
        name="store",
        compiler_params=pltpu.CompilerParams(vmem_limit_bytes=8 * 1024 * 1024),
    )(out, state)


def shards(
    tokens,
    previous,
    first_norm_gain,
    token_shift_share,
    receptance_weight,
    key_weight,
    value_weight,
    decay_down_map,
    decay_up_map,
    decay_offset,
    strength_down_map,
    strength_up_map,
    removal_key_scale,
    key_damping,
    self_term_weight,
    head_norm_gain,
    output_weight,
    state,
    second_norm_gain,
    routes,
    chosen_expert_weight,
    expert_gate_weight,
    expert_up_weight,
    expert_down_weight,
):
    gathered = gather(
        tokens, previous,
        [
            first_norm_gain.reshape(1, 2048), token_shift_share, decay_offset.reshape(1, 256),
            removal_key_scale.reshape(1, 256), key_damping.reshape(1, 256), self_term_weight,
            head_norm_gain.reshape(1, 256), second_norm_gain.reshape(1, 2048), routes.T,
            chosen_expert_weight.T, decay_down_map, strength_down_map, key_weight,
            receptance_weight, value_weight, decay_up_map, strength_up_map, state, output_weight,
        ],
    )
    return store(*layer(gathered, expert_gate_weight, expert_up_weight, expert_down_weight))


def solution(mesh):
    in_specs = (
        P("ep", "tp"),
        P("ep", "tp"),
        P(),
        P(),
        P(None, "tp"),
        P(None, "tp"),
        P(None, "tp"),
        P(),
        P(),
        P("tp"),
        P(),
        P(),
        P("tp"),
        P("tp"),
        P("tp", None),
        P("tp"),
        P("tp", None),
        P("ep", "tp", None, None),
        P(),
        P("ep", None),
        P("ep", None),
        P("ep", None, "tp"),
        P("ep", None, "tp"),
        P("ep", "tp", None),
    )
    out_specs = (P("ep", "tp"), P("ep", "tp", None, None))
    return jax.shard_map(shards, mesh=mesh, in_specs=in_specs, out_specs=out_specs, check_vma=False)
```
